256 devices in a mesh: sp: 64 (over z, y, core), tp: 4 (over x).
Axes of the slice: x: 4, y: 4, z: 8, core: 2. Of those that a mesh axis runs over, the one named last changes fastest.
Arguments:
- queries: bfloat16 [16384, 2048], P('sp', 'tp'), may hold values from -9 to 9
- keys: bfloat16 [16384, 1024], P('sp', 'tp'), may hold values from -9 to 9
- values: bfloat16 [16384, 1024], P('sp', 'tp'), may hold values from -6 to 6
- lam: float32 [8], P('tp'), may hold values from 0.3 to 0.8
- diff_gain: float32 [256], replicated, may hold values from 0.1 to 1.9
- lin_query: bfloat16 [16384, 512], P('sp', 'tp'), may hold values from -6 to 6
- lin_key: bfloat16 [16384, 512], P('sp', 'tp'), may hold values from -6 to 6
- lin_value: bfloat16 [16384, 1024], P('sp', 'tp'), may hold values from -6 to 6
- decay_pre: float32 [16384, 512], P('sp', 'tp'), may hold values from -14 to 14
- lin_gain: float32 [1024], P('tp'), may hold values from 0.1 to 1.9
- w_out_diff: bfloat16 [2048, 4096], P('tp'), may hold values from -0.125 to 0.125
- w_out_lin: bfloat16 [1024, 4096], P('tp'), may hold values from -0.1875 to 0.1875
Outputs:
- mixed: bfloat16 [16384, 4096], P(('sp', 'tp'))
The draws below stay inside these ranges and needn't reach their ends.
All inputs are finite; a program needn't handle non-finite values.
Results may differ from the reference program's by a relative error of at most 0.015.
Values may be sent and summed in bfloat16 or wider, within the bound.
No kernel may reach another device: no remote copies, remote signals or barrier semaphores. Data moves between devices by JAX's collectives and lax.ppermute only.
A program may use at most 128 MiB of HBM per device.

```python
import math
import jax
import jax.numpy as jnp
from jax import lax

D = 4096
DIFF_HEADS = 8
KV_HEADS = 4
LIN_HEADS = 4
HEAD_DIM = 128
KEY_DIM = 128
VAL_DIM = 256
BLOCK = 64
TOK_DEV = 256
SEQUENCE_TOKENS = 16384
N_TP = 4


gate_temp = 16.0


def paired_draw(key):
    query_key = jax.random.fold_in(key, 101)
    key_key = jax.random.fold_in(key, 102)
    query_shape = (SEQUENCE_TOKENS, DIFF_HEADS * 2 * HEAD_DIM)
    key_shape = (SEQUENCE_TOKENS, KV_HEADS * 2 * HEAD_DIM)
    spread = 1.32
    query_rows = jnp.clip(spread * jax.random.normal(query_key, query_shape, jnp.float32), -5.0, 5.0)
    key_rows = jnp.clip(spread * jax.random.normal(key_key, key_shape, jnp.float32), -5.0, 5.0)
    return (query_rows, key_rows)


def draw_queries(key, part):
    return paired_draw(key)[0].astype(jnp.bfloat16)


def draw_keys(key, part):
    return paired_draw(key)[1].astype(jnp.bfloat16)


def draw_decay_pre(key, part):
    width = LIN_HEADS * KEY_DIM
    random_subkeys = jax.random.split(jax.random.fold_in(key, 201), 8)
    fast_share = 0.5
    is_fast = jax.random.uniform(random_subkeys[0], (width,), jnp.float32) < fast_share
    fast_rate = jnp.exp(jax.random.uniform(random_subkeys[1], (width,), jnp.float32, math.log(0.01), math.log(1.0 / 30.0)))
    slow_rate = jnp.exp(jax.random.uniform(random_subkeys[2], (width,), jnp.float32, math.log(0.05), math.log(0.25))) / SEQUENCE_TOKENS
    decay_speed = jnp.where(is_fast, fast_rate, slow_rate)
    processor_factor = jnp.exp(jax.random.uniform(random_subkeys[3], (SEQUENCE_TOKENS // TOK_DEV,), jnp.float32, math.log(0.5), math.log(2.0)))
    processor_factor = jnp.repeat(processor_factor, TOK_DEV)[:, None]
    jaggedness = jax.random.uniform(random_subkeys[4], (SEQUENCE_TOKENS, width), jnp.float32, 0.5, 1.5)
    spike_position = jax.random.randint(random_subkeys[5], (3,), 0, SEQUENCE_TOKENS, dtype=jnp.int32)
    spike_length = jax.random.uniform(random_subkeys[6], (3,), jnp.float32, 0.22, 0.6)
    token_positions = jnp.arange(SEQUENCE_TOKENS, dtype=jnp.int32)
    spike_rows = jnp.sum(jnp.where(token_positions[:, None] == spike_position[None, :], spike_length[None, :], 0.0), axis=1)[:, None]
    logarithm_decay = -(decay_speed[None, :] * processor_factor * jaggedness) - spike_rows
    scaled = gate_temp * logarithm_decay
    return -jnp.log(jnp.expm1(-scaled))


def steps_of(stream_key, dims, cuts, low, high):
    loudness, own = 1.0, jax.random.fold_in(stream_key, 6)
    for position, parts in cuts:
        draws = jnp.exp(jax.random.uniform(jax.random.fold_in(own, position), (parts,), jnp.float32, low / len(cuts), high / len(cuts)))
        loudness = loudness * jnp.repeat(draws, dims[position] // parts).reshape([-1 if axis == position else 1 for axis in range(len(dims))])
    return loudness


def gaussian(stream_key, shape, scale, most, pieces=(), kind=jnp.bfloat16):
    drawn = scale * jax.random.normal(stream_key, shape, jnp.float32)
    if pieces:
        drawn = drawn * steps_of(stream_key, shape, pieces, -0.22, 0.18)
    return jnp.clip(drawn, -most, most).astype(kind)


def setup_inputs(seed: int = 0) -> dict:
    key_of = jax.random.split(jax.random.key(seed), 13)
    queries = draw_queries(jax.random.fold_in(key_of[12], 71), 0)
    keys = draw_keys(jax.random.fold_in(key_of[12], 71), 0)
    values = gaussian(key_of[2], (SEQUENCE_TOKENS, KV_HEADS * VAL_DIM), 1.0, 6.0, ((0, 64), (1, 4)))
    lam = jnp.clip(0.3 + 0.5 * jax.random.uniform(key_of[3], (DIFF_HEADS,), jnp.float32) ** steps_of(key_of[3], (DIFF_HEADS,), ((0, 4),), -0.2, 0.2), 0.3, 0.8)
    diff_gain = jnp.clip(1.0 + 0.18 * jax.random.normal(key_of[4], (VAL_DIM,), jnp.float32), 0.1, 1.9)
    lin_query = gaussian(key_of[5], (SEQUENCE_TOKENS, LIN_HEADS * KEY_DIM), 1.0, 6.0, ((0, 64), (1, 4)))
    lin_key = gaussian(key_of[6], (SEQUENCE_TOKENS, LIN_HEADS * KEY_DIM), 1.0, 6.0, ((0, 64), (1, 4)))
    lin_value = gaussian(key_of[7], (SEQUENCE_TOKENS, LIN_HEADS * VAL_DIM), 1.0, 6.0, ((0, 64), (1, 4)))
    decay_pre = draw_decay_pre(jax.random.fold_in(key_of[12], 71), 0)
    lin_gain = jnp.clip(1.0 + 0.18 * jax.random.normal(key_of[9], (LIN_HEADS * VAL_DIM,), jnp.float32), 0.1, 1.9)
    w_out_diff = gaussian(key_of[10], (DIFF_HEADS * VAL_DIM, D), (DIFF_HEADS * VAL_DIM) ** -0.5, 0.125, ((0, 4),))
    w_out_lin = gaussian(key_of[11], (LIN_HEADS * VAL_DIM, D), (LIN_HEADS * VAL_DIM) ** -0.5, 0.1875, ((0, 4),))
    return {"queries": queries, "keys": keys, "values": values, "lam": lam, "diff_gain": diff_gain, "lin_query": lin_query, "lin_key": lin_key, "lin_value": lin_value, "decay_pre": decay_pre, "lin_gain": lin_gain, "w_out_diff": w_out_diff, "w_out_lin": w_out_lin}


norm_eps = 1e-06
gate_temp = 16.0
neg_large = -1e+30
highest = lax.Precision.HIGHEST

def head_norm(mixed_in, gain):
    return mixed_in * lax.rsqrt(lax.optimization_barrier(jnp.mean(mixed_in * mixed_in, axis=-1, keepdims=True)) + norm_eps) * gain

def one_map(query_rows, key_rows, value_rows, query_pos, key_pos):
    scores = jnp.einsum('jqd,sd->jqs', query_rows, key_rows) / math.sqrt(HEAD_DIM)
    allowed = query_pos[:, None] >= key_pos[None, :]
    scores = jnp.where(allowed, scores, neg_large)
    row_top = lax.optimization_barrier(jnp.max(scores, axis=-1, keepdims=True))
    expo = jnp.where(allowed, jnp.exp(scores - row_top), 0.0)
    totals = lax.optimization_barrier(jnp.sum(expo, axis=-1))
    weights = lax.optimization_barrier(expo.astype(jnp.bfloat16)).astype(jnp.float32)
    numer = jnp.einsum('jqs,se->jqe', weights, value_rows)
    return numer / totals[..., None]

def diff_attention(queries, keys, values, lam, diff_gain):
    group_size = DIFF_HEADS // KV_HEADS
    query_all = queries.astype(jnp.float32).reshape(SEQUENCE_TOKENS, KV_HEADS, group_size, 2, HEAD_DIM)
    key_all = keys.astype(jnp.float32).reshape(SEQUENCE_TOKENS, KV_HEADS, 2, HEAD_DIM)
    value_all = values.astype(jnp.float32).reshape(SEQUENCE_TOKENS, KV_HEADS, VAL_DIM)
    lam_grid = lam.reshape(KV_HEADS, group_size)
    span_rows = math.gcd(SEQUENCE_TOKENS, 1024)
    outputs = []
    for block_index in range(SEQUENCE_TOKENS // span_rows):
        begin = block_index * span_rows
        limit = begin + span_rows
        query_pos = begin + jnp.arange(span_rows, dtype=jnp.int32)
        key_pos = jnp.arange(limit, dtype=jnp.int32)
        query_rows = query_all[begin:limit].transpose(1, 2, 3, 0, 4)
        key_rows = key_all[:limit].transpose(1, 2, 0, 3)
        value_rows = value_all[:limit].transpose(1, 0, 2)

        def per_group(operands):
            query_group, key_group, value_group, lam_group = operands
            first_out = one_map(query_group[:, 0], key_group[0], value_group, query_pos, key_pos)
            second_out = one_map(query_group[:, 1], key_group[1], value_group, query_pos, key_pos)
            return first_out - lam_group[:, None, None] * second_out
        attended = lax.map(per_group, (query_rows, key_rows, value_rows, lam_grid))
        normed = head_norm(attended, diff_gain).astype(jnp.bfloat16)
        outputs.append(normed.transpose(2, 0, 1, 3).reshape(span_rows, DIFF_HEADS * VAL_DIM))
    return jnp.concatenate(outputs, axis=0)

def gla_step(run_state, inputs):
    query_blk, key_blk, value_blk, decay_blk = inputs
    length = query_blk.shape[1]
    cumulative = jnp.cumsum(decay_blk, axis=1)
    lower_mask = jnp.tril(jnp.ones((length, length), dtype=bool))[None, :, :, None]
    spread = jnp.where(lower_mask, cumulative[:, :, None, :] - cumulative[:, None, :, :], 0.0)
    factor = jnp.where(lower_mask, jnp.exp(spread), 0.0)
    inner = jnp.einsum('htd,hsd,htsd->hts', query_blk, key_blk, factor, precision=highest)
    local_part = jnp.einsum('hts,hse->hte', inner, value_blk, precision=highest)
    carried = jnp.einsum('htd,hde->hte', query_blk * jnp.exp(cumulative), run_state, precision=highest)
    last_sum = cumulative[:, -1:, :]
    new_state = jnp.exp(last_sum[:, 0, :])[..., None] * run_state + jnp.einsum('hsd,hse->hde', key_blk * jnp.exp(last_sum - cumulative), value_blk, precision=highest)
    return (new_state, local_part + carried)

def linear_attention(lin_query, lin_key, lin_value, decay_pre, lin_gain):
    block_count = SEQUENCE_TOKENS // BLOCK

    def arrange(array, width):
        return array.astype(jnp.float32).reshape(block_count, BLOCK, LIN_HEADS, width).transpose(0, 2, 1, 3)
    start_state = jnp.zeros((LIN_HEADS, KEY_DIM, VAL_DIM), jnp.float32)
    _, outputs = lax.scan(gla_step, start_state, (arrange(lin_query, KEY_DIM) * KEY_DIM ** (-0.5), arrange(lin_key, KEY_DIM), arrange(lin_value, VAL_DIM), arrange(jax.nn.log_sigmoid(decay_pre) / gate_temp, KEY_DIM)))
    linear_rows = outputs.transpose(0, 2, 1, 3).reshape(SEQUENCE_TOKENS, LIN_HEADS, VAL_DIM)
    normed = head_norm(linear_rows, lin_gain.reshape(LIN_HEADS, VAL_DIM)).astype(jnp.bfloat16)
    return normed.reshape(SEQUENCE_TOKENS, LIN_HEADS * VAL_DIM)

def reference(queries, keys, values, lam, diff_gain, lin_query, lin_key, lin_value, decay_pre, lin_gain, w_out_diff, w_out_lin):
    diff_out = diff_attention(queries, keys, values, lam, diff_gain)
    lin_out = linear_attention(lin_query, lin_key, lin_value, decay_pre, lin_gain)
    diff_cols = DIFF_HEADS * VAL_DIM // N_TP
    lin_cols = LIN_HEADS * VAL_DIM // N_TP
    summed = jnp.zeros((SEQUENCE_TOKENS, D), jnp.float32)
    for member in range(N_TP):
        diff_lo = member * diff_cols
        lin_lo = member * lin_cols
        partial_value = jnp.dot(diff_out[:, diff_lo:diff_lo + diff_cols], w_out_diff[diff_lo:diff_lo + diff_cols], preferred_element_type=jnp.float32)
        partial_value = partial_value + jnp.dot(lin_out[:, lin_lo:lin_lo + lin_cols], w_out_lin[lin_lo:lin_lo + lin_cols], preferred_element_type=jnp.float32)
        partial_value = lax.optimization_barrier(partial_value.astype(jnp.bfloat16)).astype(jnp.float32)
        summed = summed + partial_value
    return summed.astype(jnp.bfloat16)
```

```python
import functools
import math

import jax
import jax.numpy as jnp
from jax import lax
from jax.experimental import pallas as pl
from jax.experimental.pallas import tpu as pltpu
from jax.sharding import Mesh
from jax.sharding import PartitionSpec as P

HEAD_DIM = 128
KEY_DIM = 128
VAL_DIM = 256
NZ, NY, NX = 8, 4, 4
TOK = 256
HALF = 128
CHIPS = NZ * NY
SP = ("z", "y", "c")
EPS = 1e-6
NEG = -1e30
LOG2E = 1.4426950408889634
SCORE = LOG2E / math.sqrt(HEAD_DIM)
F32 = jnp.float32
BF16 = jnp.bfloat16


NT = (((1,), (1,)), ((), ()))
TN = (((0,), (0,)), ((), ()))


def vmem():
    return pl.BlockSpec(memory_space=pltpu.VMEM)


def smem():
    return pl.BlockSpec(memory_space=pltpu.SMEM)


def params(**kw):
    return pltpu.CompilerParams(**kw)


def place(z, y, c):
    return (z % NZ) * 8 + (y % NY) * 2 + c


def moved(a, zero=None, one=None):
    pairs = []
    for c, step in ((0, zero), (1, one)):
        if step is not None:
            for z in range(NZ):
                for y in range(NY):
                    pairs.append((place(z, y, c), place(z + step[0], y + step[1], c)))
    return lax.ppermute(a, SP, pairs)


def swap(a):
    return lax.ppermute(a, "c", [(0, 1), (1, 0)])


def chip_ahead(a, d):
    return lax.ppermute(a, ("z", "y"), [(i, i + d) for i in range(CHIPS - d)])


def any_space():
    return pl.BlockSpec(memory_space=pl.ANY)


def join_kernel(plans, n_in, me_ref, *refs):
    ins, outs, sems = refs[:n_in], refs[n_in:-1], refs[-1]

    def run(plan):
        copies = [
            pltpu.make_async_copy(ins[i], outs[o].at[rows, cols], sems.at[k])
            for k, (i, o, rows, cols) in enumerate(plan)
        ]
        for copy in copies:
            copy.start()
        for copy in copies:
            copy.wait()

    if len(plans) == 1:
        run(plans[0])
    else:
        c = me_ref[0] & 1
        for which, plan in enumerate(plans):
            pl.when(c == which)(functools.partial(run, plan))


def join(me, ins, n_out, rows, plans):
    out = jax.ShapeDtypeStruct((rows, 512), BF16)
    return pl.pallas_call(
        functools.partial(join_kernel, plans, len(ins)),
        out_shape=(out,) * n_out,
        in_specs=[smem(), *[any_space()] * len(ins)],
        out_specs=(vmem(),) * n_out,
        scratch_shapes=[pltpu.SemaphoreType.DMA((max(map(len, plans)),))],
        cost_estimate=small_cost(),
        name="join",
    )(me, *ins)


def linear_kernel(q_ref, k_ref, v_ref, d_ref, rows_ref, reach_ref, state_ref, send_ref):
    n = HALF
    row = lax.broadcasted_iota(jnp.int32, (n, n), 0)
    col = lax.broadcasted_iota(jnp.int32, (n, n), 1)
    lower = row >= col
    tri = jnp.where(lower, 1.0, 0.0).astype(F32)
    state = None
    passed = jnp.zeros((1, KEY_DIM), F32)
    for part in range(TOK // n):
        sl = pl.ds(part * n, n)
        pre = d_ref[sl, :]
        decay = (jnp.minimum(pre, 0.0) - jnp.log1p(jnp.exp(-jnp.abs(pre)))) / 16.0
        total = jnp.dot(tri, decay, precision=lax.Precision.HIGHEST, preferred_element_type=F32)
        mid = total[n // 2 - 1 : n // 2, :]
        last = total[n - 1 : n, :]
        q = q_ref[sl, :].astype(F32) * KEY_DIM**-0.5
        k = k_ref[sl, :].astype(F32)
        v = v_ref[sl, :]
        inner = lax.dot_general(
            (q * jnp.exp(total - mid)).astype(BF16),
            (k * jnp.exp(mid - total)).astype(BF16),
            NT,
            preferred_element_type=F32,
        )
        inner = jnp.where(lower, inner, 0.0)
        rows = jnp.dot(inner.astype(BF16), v, preferred_element_type=F32)
        added = lax.dot_general(
            v, (k * jnp.exp(last - total)).astype(BF16), TN, preferred_element_type=F32
        )
        if state is None:
            state = added
        else:
            rows = rows + lax.dot_general(
                (q * jnp.exp(total)).astype(BF16),
                state.astype(BF16),
                NT,
                preferred_element_type=F32,
            )
            state = state * jnp.exp(last) + added
        rows_ref[sl, :] = rows
        reach_ref[sl, :] = (q * jnp.exp(passed + total)).astype(BF16)
        passed = passed + last
    write_state(state, passed, state_ref, send_ref)


def write_state(state, passed, state_ref, send_ref):
    if state_ref is not None:
        state_ref[0:VAL_DIM, :] = state
        state_ref[VAL_DIM:, :] = jnp.broadcast_to(passed, (8, KEY_DIM))
    if send_ref is not None:
        high = passed.astype(BF16)
        low = (passed - high.astype(F32)).astype(BF16)
        send_ref[0:VAL_DIM, :] = state.astype(BF16)
        at = lax.broadcasted_iota(jnp.int32, (16, KEY_DIM), 0)
        both = jnp.where(at == 0, high.astype(F32), jnp.where(at == 1, low.astype(F32), 0.0))
        send_ref[VAL_DIM:, :] = both.astype(BF16)


def read_sent(ref):
    state = ref[0:VAL_DIM, :].astype(F32)
    tail = ref[VAL_DIM:, :].astype(F32)
    return state, tail[0:1, :] + tail[1:2, :]


def read_state(ref):
    return ref[0:VAL_DIM, :], ref[VAL_DIM : VAL_DIM + 1, :]


def chain(earlier, later):
    return jnp.exp(later[1]) * earlier[0] + later[0], earlier[1] + later[1]


STATE = jax.ShapeDtypeStruct((VAL_DIM + 8, KEY_DIM), F32)
SENT = jax.ShapeDtypeStruct((VAL_DIM + 16, KEY_DIM), BF16)


def linear_local(q, k, v, d):
    return pl.pallas_call(
        linear_kernel,
        out_shape=(
            jax.ShapeDtypeStruct((TOK, VAL_DIM), F32),
            jax.ShapeDtypeStruct((TOK, KEY_DIM), BF16),
            STATE,
            SENT,
        ),
        in_specs=[vmem()] * 4,
        out_specs=(vmem(),) * 4,
        cost_estimate=pl.CostEstimate(
            flops=3_000_000_000, bytes_accessed=800_000, transcendentals=0
        ),
        name="linear_local",
    )(q, k, v, d)


def pair_kernel(me_ref, own_ref, got_ref, all_ref, before_ref, send_ref):
    second = (me_ref[0] & 1) == 1
    own, got = read_state(own_ref), read_sent(got_ref)
    first_s = jnp.where(second, got[0], own[0])
    first_d = jnp.where(second, got[1], own[1])
    later_s = jnp.where(second, own[0], got[0])
    later_d = jnp.where(second, own[1], got[1])
    state, passed = chain((first_s, first_d), (later_s, later_d))
    write_state(state, passed, all_ref, send_ref)
    write_state(
        jnp.where(second, got[0], 0.0), jnp.where(second, got[1], 0.0), before_ref, None
    )


def step_kernel(all_ref, before_ref, got_ref, new_all_ref, new_before_ref, send_ref):
    got = read_sent(got_ref)
    state, passed = chain(got, read_state(all_ref))
    write_state(state, passed, new_all_ref, send_ref)
    state, passed = chain(got, read_state(before_ref))
    write_state(state, passed, new_before_ref, None)


def small_cost():
    return pl.CostEstimate(flops=500_000_000, bytes_accessed=500_000, transcendentals=0)


def pair_state(me, own, got):
    return pl.pallas_call(
        pair_kernel,
        out_shape=(STATE, STATE, SENT),
        in_specs=[smem(), vmem(), vmem()],
        out_specs=(vmem(),) * 3,
        cost_estimate=small_cost(),
        name="pair_state",
    )(me, own, got)


def step_state(whole, before, got):
    return pl.pallas_call(
        step_kernel,
        out_shape=(STATE, STATE, SENT),
        in_specs=[vmem()] * 3,
        out_specs=(vmem(),) * 3,
        cost_estimate=small_cost(),
        name="step_state",
    )(whole, before, got)


ROWS = 2 * TOK
WIDE = 4 * TOK


def attend_kernel(tables, first, off, n_buf, me_ref, qo_ref, qw_ref, *refs):
    bufs = refs[:n_buf]
    if first:
        acc_ref, stat_ref, q_ref, kv_ref, top_ref, part_ref, flag_ref, sems = refs[n_buf:]
    else:
        acc_in, stat_in, acc_ref, stat_ref, q_ref, kv_ref, top_ref, part_ref, flag_ref, sems = refs[
            n_buf:
        ]
    tile = pl.program_id(0) + off
    lead = pl.program_id(0) == 0
    me = me_ref[0]
    z, y, c = me >> 3, (me >> 1) & 3, me & 1
    chip = z * NY + y
    n_group = len(tables)
    pieces = len(tables[0][0])

    def fetches(g):
        if first:
            return [pltpu.make_async_copy(bufs[0], kv_ref.at[0], sems.at[0])]
        per = n_buf // n_group
        rows = WIDE // per
        return [
            pltpu.make_async_copy(
                bufs[g * per + i], kv_ref.at[g, pl.ds(i * rows, rows)], sems.at[g * per + i]
            )
            for i in range(per)
        ]

    @pl.when(lead)
    def _():
        for g, (zero, one) in enumerate(tables):
            for i in range(pieces):
                dz = jnp.where(c == 0, zero[i][0], one[i][0])
                dy = jnp.where(c == 0, zero[i][1], one[i][1])
                source = ((z + dz) & (NZ - 1)) * NY + ((y + dy) & (NY - 1))
                flag_ref[g * pieces + i] = (source < chip).astype(jnp.int32)
            for copy in fetches(g):
                copy.start()

    @pl.when(tile == 0)
    def _():
        q_ref[0:TOK, :] = qo_ref[:, 0:256]
        q_ref[TOK:ROWS, :] = qo_ref[:, 256:512]

    @pl.when(tile == 1)
    def _():
        q_ref[0:TOK, :] = qw_ref[:, 0:256]
        q_ref[TOK:ROWS, :] = qw_ref[:, 256:512]

    lane = lax.broadcasted_iota(jnp.int32, (ROWS, 128), 1)
    if first:
        acc_ref[...] = jnp.zeros_like(acc_ref)
        top_ref[...] = jnp.full(top_ref.shape, NEG, F32)
        part_ref[...] = jnp.zeros_like(part_ref)
    else:
        acc_ref[...] = acc_in[...]
        for mp in range(2):
            top_ref[mp] = jnp.broadcast_to(stat_in[:, mp : mp + 1], (ROWS, 128))
            part_ref[mp] = jnp.where(lane == 0, stat_in[:, 2 + mp : 3 + mp], 0.0)

    def visit(g, lo, n, bias=None, allowed=None):
        scores = [
            lax.dot_general(
                q_ref[:, mp * 128 : mp * 128 + 128],
                kv_ref[g, lo : lo + n, mp * 128 : mp * 128 + 128],
                NT,
                preferred_element_type=F32,
            )
            for mp in range(2)
        ]
        v = kv_ref[g, lo : lo + n, 256:512]
        for mp in range(2):
            s = scores[mp]
            if bias is not None:
                s = s + bias
            if allowed is not None:
                s = jnp.where(allowed, s, NEG)
            old = top_ref[mp]
            new = jnp.maximum(old, jnp.max(s, axis=-1, keepdims=True))
            weights, part = [], None
            for j in range(n // 128):
                w = jnp.exp2((s[:, j * 128 : j * 128 + 128] - new) * SCORE)
                part = w if part is None else part + w
                weights.append(w.astype(BF16))
            shrink = jnp.exp2((old - new) * SCORE)
            part_ref[mp] = part_ref[mp] * shrink + part
            top_ref[mp] = new
            added = jnp.dot(
                jnp.concatenate(weights, axis=1), v, preferred_element_type=F32
            )
            for j in range(2):
                cols = slice(mp * 256 + j * 128, mp * 256 + j * 128 + 128)
                acc_ref[:, cols] = acc_ref[:, cols] * shrink + added[:, j * 128 : j * 128 + 128]

    def group(g, lo, n):
        flags = [flag_ref[g * pieces + i] for i in range(pieces)]
        count = functools.reduce(jnp.add, flags)

        @pl.when(count == pieces)
        def _():
            visit(g, lo, n)

        @pl.when((count > 0) & (count < pieces))
        def _():
            at = lax.broadcasted_iota(jnp.int32, (1, n), 1)
            bias = jnp.zeros((1, n), F32)
            size = n // pieces
            for i, ok in enumerate(flags):
                here = (at >= i * size) & (at < (i + 1) * size)
                bias = jnp.where(here & (ok == 0), NEG, bias)
            visit(g, lo, n, bias=bias)

    def wait(g):
        @pl.when(lead)
        def _():
            for copy in fetches(g):
                copy.wait()

    if first:
        wait(0)
        qb = jnp.where(tile == 0, 1 - c, c)
        row = lax.broadcasted_iota(jnp.int32, (ROWS, TOK), 0) & (TOK - 1)
        col = lax.broadcasted_iota(jnp.int32, (ROWS, TOK), 1)
        visit(0, 0, TOK, allowed=qb * TOK + row >= c * TOK + col)
        group(0, TOK, pieces * TOK)
    else:
        for g in range(n_group):
            wait(g)
        if n_group == 1:
            group(0, 0, WIDE)
        else:

            def loop(g, carry):
                group(g, 0, WIDE)
                return carry

            lax.fori_loop(0, n_group, loop, 0)

    stat_ref[...] = jnp.where(
        lane == 0,
        top_ref[0],
        jnp.where(
            lane == 1,
            top_ref[1],
            jnp.where(
                lane == 2,
                jnp.sum(part_ref[0], axis=-1, keepdims=True),
                jnp.sum(part_ref[1], axis=-1, keepdims=True),
            ),
        ),
    )


def attend(me, qo, qw, bufs, tables, state=None, off=0, tiles=2):
    first = state is None
    n_group = len(tables)
    keys = WIDE * n_group
    acc = lambda o: pl.BlockSpec((ROWS, 512), lambda t: (t + o, 0))
    stat = lambda o: pl.BlockSpec((ROWS, 128), lambda t: (t + o, 0))
    return pl.pallas_call(
        functools.partial(attend_kernel, tables, first, off, len(bufs)),
        grid=(tiles,),
        out_shape=(
            jax.ShapeDtypeStruct((tiles * ROWS, 512), F32),
            jax.ShapeDtypeStruct((tiles * ROWS, 128), F32),
        ),
        in_specs=[
            smem(),
            vmem(),
            vmem(),
            *[any_space()] * len(bufs),
            *([] if first else [acc(off), stat(off)]),
        ],
        out_specs=(acc(0), stat(0)),
        scratch_shapes=[
            pltpu.VMEM((ROWS, 256), BF16),
            pltpu.VMEM((n_group, WIDE, 512), BF16),
            pltpu.VMEM((2, ROWS, 128), F32),
            pltpu.VMEM((2, ROWS, 128), F32),
            pltpu.SMEM((n_group * len(tables[0][0]),), jnp.int32),
            pltpu.SemaphoreType.DMA((len(bufs),)),
        ],
        compiler_params=params(dimension_semantics=("arbitrary",)),
        cost_estimate=pl.CostEstimate(
            flops=2 * tiles * ROWS * keys * 2 * (256 + 256),
            bytes_accessed=4_000_000,
            transcendentals=0,
        ),
        name="attend",
    )(me, qo, qw, *bufs, *(() if first else state))


CUTS = 8


def head_norm(x, gain):
    return x * lax.rsqrt(jnp.mean(x * x, axis=-1, keepdims=True) + EPS) * gain


def project_kernel(
    lam_ref, acc_hbm, oacc_hbm, wd_hbm, wl_hbm, stat_ref, ostat_ref, dg_ref, rows_ref, reach_ref,
    before_ref, got_ref, lg_ref, out_hbm, acc_ref, oacc_ref, w_ref, x_ref, o_ref, sems,
):
    width = w_ref.shape[1] // CUTS
    load = [
        pltpu.make_async_copy(acc_hbm, acc_ref, sems.at[0]),
        pltpu.make_async_copy(oacc_hbm, oacc_ref, sems.at[1]),
    ]
    weights = []
    for j in range(CUTS):
        cols = pl.ds(j * width, width)
        weights.append(
            (
                pltpu.make_async_copy(
                    wd_hbm.at[:, cols], w_ref.at[0:512, cols], sems.at[2 + 2 * j]
                ),
                pltpu.make_async_copy(
                    wl_hbm.at[:, cols], w_ref.at[512:768, cols], sems.at[3 + 2 * j]
                ),
            )
        )
    for copy in load:
        copy.start()
    for pair in weights:
        for copy in pair:
            copy.start()
    incoming, _ = chain(read_sent(got_ref), read_state(before_ref))
    linear = rows_ref[...] + lax.dot_general(
        reach_ref[...], incoming.astype(BF16), NT, preferred_element_type=F32
    )
    x_ref[:, 512:768] = head_norm(linear, lg_ref[...]).astype(BF16)
    for copy in load:
        copy.wait()
    for h in range(2):
        maps = []
        part = slice(h * TOK, h * TOK + TOK)
        for mp in range(2):
            top_a, top_b = stat_ref[part, mp : mp + 1], ostat_ref[part, mp : mp + 1]
            top = jnp.maximum(top_a, top_b)
            sa = jnp.exp2((top_a - top) * SCORE)
            sb = jnp.exp2((top_b - top) * SCORE)
            total = stat_ref[part, 2 + mp : 3 + mp] * sa + ostat_ref[part, 2 + mp : 3 + mp] * sb
            cols = slice(mp * 256, mp * 256 + 256)
            maps.append(acc_ref[part, cols] * (sa / total) + oacc_ref[part, cols] * (sb / total))
        attended = maps[0] - lam_ref[h] * maps[1]
        x_ref[:, h * 256 : h * 256 + 256] = head_norm(attended, dg_ref[...]).astype(BF16)
    stores = []
    for j, pair in enumerate(weights):
        for copy in pair:
            copy.wait()
        cols = slice(j * width, j * width + width)
        o_ref[j] = jnp.dot(x_ref[...], w_ref[:, cols], preferred_element_type=F32).astype(BF16)
        store = pltpu.make_async_copy(
            o_ref.at[j], out_hbm.at[:, pl.ds(j * width, width)], sems.at[2 + 2 * CUTS + j]
        )
        store.start()
        stores.append(store)
    for store in stores:
        store.wait()


def project(lam, state, other, dg, rows, reach, before, got, lg, wd, wl):
    model = wd.shape[1]
    return pl.pallas_call(
        project_kernel,
        out_shape=jax.ShapeDtypeStruct((TOK, model), BF16),
        in_specs=[smem(), *[any_space()] * 4, *[vmem()] * 8],
        out_specs=any_space(),
        scratch_shapes=[
            pltpu.VMEM((ROWS, 512), F32),
            pltpu.VMEM((ROWS, 512), F32),
            pltpu.VMEM((768, model), BF16),
            pltpu.VMEM((TOK, 768), BF16),
            pltpu.VMEM((CUTS, TOK, model // CUTS), BF16),
            pltpu.SemaphoreType.DMA((2 + 3 * CUTS,)),
        ],
        cost_estimate=pl.CostEstimate(
            flops=2 * TOK * 768 * model, bytes_accessed=12_000_000, transcendentals=0
        ),
        name="project",
    )(lam, state[0], other[0], wd, wl, state[1], other[1], dg, rows, reach, before, got, lg)


ROW = (0, -1, 1, -2)
NEAR = (0, -1, 1, -2)
FAR = (2, -3, 3, 4)


def body(
    queries, keys, values, lam, diff_gain, lin_query, lin_key, lin_value,
    decay_pre, lin_gain, w_out_diff, w_out_lin,
):
    me = lax.axis_index(SP).astype(jnp.int32).reshape(1)
    tied = lax.optimization_barrier
    every = slice(None)
    span = lambda k: pl.ds(k * TOK, TOK)
    (kv,) = join(
        me,
        (keys, values),
        1,
        TOK,
        (((0, 0, every, pl.ds(0, 256)), (1, 0, every, pl.ds(256, 256))),),
    )
    zp, zm, yp, ym = (1, 0), (-1, 0), (0, 1), (0, -1)

    p1, m1 = moved(kv, zp, yp), moved(kv, zm, ym)
    q_other = swap(queries)
    rows, reach, own_state, sent = linear_local(lin_query, lin_key, lin_value, decay_pre)
    p1, m1, q_other, own_state, sent = tied((p1, m1, q_other, own_state, sent))

    p2, m2 = moved(p1, zp, yp), moved(m1, zm, None)
    got = swap(sent)
    p2, m2, got = tied((p2, m2, got))

    (near,) = join(
        me,
        (kv, p1, m1, p2),
        1,
        WIDE,
        (tuple((i, 0, span(i), every) for i in range(4)),),
    )
    p3, m3 = moved(near, yp, zp), moved(near, ym, zm)
    xm3, xp3 = moved(p2, zp, None), moved(m2, zm, None)
    whole, before, sent = pair_state(me, own_state, got)
    got = chip_ahead(sent, 1)
    state = attend(
        me,
        q_other,
        queries,
        (near,),
        ((tuple((dz, 0) for dz in NEAR[1:]), tuple((0, dy) for dy in ROW[1:])),),
    )
    p3, m3, xm3, xp3, got, state = tied((p3, m3, xm3, xp3, got, state))

    p4, m4 = moved(p3, yp, zp), moved(m3, None, zm)
    x4 = moved(xm3, zp, None)
    whole, before, sent = step_state(whole, before, got)
    got = chip_ahead(sent, 2)
    state = attend(
        me,
        q_other,
        queries,
        (p3, m3),
        (
            (tuple((dz, -1) for dz in NEAR), tuple((-1, dy) for dy in ROW)),
            (tuple((dz, 1) for dz in NEAR), tuple((1, dy) for dy in ROW)),
        ),
        state,
    )
    p4, m4, x4, got, state = tied((p4, m4, x4, got, state))

    far_p, far_m = join(
        me,
        (m2, xm3, xp3, x4, p4, m4),
        2,
        WIDE,
        (
            tuple((i, o, span(i), every) for o in range(2) for i in range(4)),
            ((4, 0, every, every), (5, 1, every, every)),
        ),
    )
    p5, m5 = moved(far_p, yp, zp), moved(far_m, ym, zm)
    whole, before, sent = step_state(whole, before, got)
    got = chip_ahead(sent, 4)
    state = attend(
        me,
        q_other,
        queries,
        (p4, far_m),
        (
            (tuple((dz, -2) for dz in NEAR), tuple((-2, dy) for dy in ROW)),
            (tuple((dz, 0) for dz in FAR), tuple((2, dy) for dy in ROW)),
        ),
        state,
    )
    p5, m5, got, state = tied((p5, m5, got, state))

    p6, m6 = moved(p5[: 2 * TOK], yp, zp), moved(m5[2 * TOK :], ym, zm)
    whole, before, sent = step_state(whole, before, got)
    got = chip_ahead(sent, 8)
    state = attend(
        me,
        q_other,
        queries,
        (p5, m5),
        (
            (tuple((dz, -1) for dz in FAR), tuple((-3, dy) for dy in ROW)),
            (tuple((dz, 1) for dz in FAR), tuple((3, dy) for dy in ROW)),
        ),
        state,
    )
    p6, m6, got, state = tied((p6, m6, got, state))

    whole, before, sent = step_state(whole, before, got)
    got = chip_ahead(sent, 16)
    tail = (
        (p6, m6),
        ((tuple((dz, 2) for dz in FAR), tuple((4, dy) for dy in ROW)),),
    )
    theirs = attend(me, q_other, queries, *tail, state, off=0, tiles=1)
    other = tuple(swap(a) for a in theirs)
    mine = attend(me, q_other, queries, *tail, state, off=1, tiles=1)
    partial = project(
        lam, mine, other, diff_gain.reshape(1, -1), rows, reach, before, got,
        lin_gain.reshape(1, -1), w_out_diff, w_out_lin,
    )
    blocks = partial.reshape(NX, TOK // NX, partial.shape[1])
    arrived = lax.all_to_all(blocks, "tp", split_axis=0, concat_axis=0, tiled=True)
    return arrived.astype(F32).sum(axis=0).astype(BF16)


def solution(mesh):
    finer = Mesh(mesh.devices.reshape(NZ, NY, 2, mesh.shape["tp"]), ("z", "y", "c", "tp"))
    in_specs = (
        P(SP, "tp"),
        P(SP, "tp"),
        P(SP, "tp"),
        P("tp"),
        P(),
        P(SP, "tp"),
        P(SP, "tp"),
        P(SP, "tp"),
        P(SP, "tp"),
        P("tp"),
        P("tp", None),
        P("tp", None),
    )
    out_specs = P((*SP, "tp"), None)
    return jax.shard_map(body, mesh=finer, in_specs=in_specs, out_specs=out_specs, check_vma=False)
```

```python
import functools
import math

import jax
import jax.numpy as jnp
from jax import lax
from jax.experimental import pallas as pl
from jax.experimental.pallas import tpu as pltpu
from jax.sharding import Mesh
from jax.sharding import PartitionSpec as P

HEAD_DIM = 128
KEY_DIM = 128
VAL_DIM = 256
NZ, NY, NX = 8, 4, 4
TOK = 256
HALF = 128
CHIPS = NZ * NY
SP = ("z", "y", "c")
EPS = 1e-6
NEG = -1e30
LOG2E = 1.4426950408889634
SCORE = LOG2E / math.sqrt(HEAD_DIM)
F32 = jnp.float32
BF16 = jnp.bfloat16


NT = (((1,), (1,)), ((), ()))
TN = (((0,), (0,)), ((), ()))


def vmem():
    return pl.BlockSpec(memory_space=pltpu.VMEM)


def smem():
    return pl.BlockSpec(memory_space=pltpu.SMEM)


def params(mib, **kw):
    return pltpu.CompilerParams(vmem_limit_bytes=mib * 2**20, **kw)


def place(z, y, c):
    return (z % NZ) * 8 + (y % NY) * 2 + c


def moved(a, zero=None, one=None):
    pairs = []
    for c, step in ((0, zero), (1, one)):
        if step is not None:
            for z in range(NZ):
                for y in range(NY):
                    pairs.append((place(z, y, c), place(z + step[0], y + step[1], c)))
    return lax.ppermute(a, SP, pairs)


def swap(a):
    return lax.ppermute(a, "c", [(0, 1), (1, 0)])


def chip_ahead(a, d):
    return lax.ppermute(a, ("z", "y"), [(i, i + d) for i in range(CHIPS - d)])


def any_space():
    return pl.BlockSpec(memory_space=pl.ANY)


def join_kernel(plans, n_in, me_ref, *refs):
    ins, outs, sems = refs[:n_in], refs[n_in:-1], refs[-1]

    def run(plan):
        copies = [
            pltpu.make_async_copy(ins[i], outs[o].at[rows, cols], sems.at[k])
            for k, (i, o, rows, cols) in enumerate(plan)
        ]
        for copy in copies:
            copy.start()
        for copy in copies:
            copy.wait()

    if len(plans) == 1:
        run(plans[0])
    else:
        c = me_ref[0] & 1
        for which, plan in enumerate(plans):
            pl.when(c == which)(functools.partial(run, plan))


def join(me, ins, n_out, rows, plans):
    out = jax.ShapeDtypeStruct((rows, 512), BF16)
    return pl.pallas_call(
        functools.partial(join_kernel, plans, len(ins)),
        out_shape=(out,) * n_out,
        in_specs=[smem(), *[any_space()] * len(ins)],
        out_specs=(vmem(),) * n_out,
        scratch_shapes=[pltpu.SemaphoreType.DMA((max(map(len, plans)),))],
        compiler_params=params(8),
        cost_estimate=small_cost(),
        name="join",
    )(me, *ins)


def linear_kernel(q_ref, k_ref, v_ref, d_ref, rows_ref, reach_ref, state_ref, send_ref):
    n = HALF
    row = lax.broadcasted_iota(jnp.int32, (n, n), 0)
    col = lax.broadcasted_iota(jnp.int32, (n, n), 1)
    lower = row >= col
    tri = jnp.where(lower, 1.0, 0.0).astype(F32)
    state = None
    passed = jnp.zeros((1, KEY_DIM), F32)
    for part in range(TOK // n):
        sl = pl.ds(part * n, n)
        pre = d_ref[sl, :]
        decay = (jnp.minimum(pre, 0.0) - jnp.log1p(jnp.exp(-jnp.abs(pre)))) / 16.0
        total = jnp.dot(tri, decay, precision=lax.Precision.HIGHEST, preferred_element_type=F32)
        mid = total[n // 2 - 1 : n // 2, :]
        last = total[n - 1 : n, :]
        q = q_ref[sl, :].astype(F32) * KEY_DIM**-0.5
        k = k_ref[sl, :].astype(F32)
        v = v_ref[sl, :]
        inner = lax.dot_general(
            (q * jnp.exp(total - mid)).astype(BF16),
            (k * jnp.exp(mid - total)).astype(BF16),
            NT,
            preferred_element_type=F32,
        )
        inner = jnp.where(lower, inner, 0.0)
        rows = jnp.dot(inner.astype(BF16), v, preferred_element_type=F32)
        added = lax.dot_general(
            v, (k * jnp.exp(last - total)).astype(BF16), TN, preferred_element_type=F32
        )
        if state is None:
            state = added
        else:
            rows = rows + lax.dot_general(
                (q * jnp.exp(total)).astype(BF16),
                state.astype(BF16),
                NT,
                preferred_element_type=F32,
            )
            state = state * jnp.exp(last) + added
        rows_ref[sl, :] = rows
        reach_ref[sl, :] = (q * jnp.exp(passed + total)).astype(BF16)
        passed = passed + last
    write_state(state, passed, state_ref, send_ref)


def write_state(state, passed, state_ref, send_ref):
    if state_ref is not None:
        state_ref[0:VAL_DIM, :] = state
        state_ref[VAL_DIM:, :] = jnp.broadcast_to(passed, (8, KEY_DIM))
    if send_ref is not None:
        high = passed.astype(BF16)
        low = (passed - high.astype(F32)).astype(BF16)
        send_ref[0:VAL_DIM, :] = state.astype(BF16)
        at = lax.broadcasted_iota(jnp.int32, (16, KEY_DIM), 0)
        both = jnp.where(at == 0, high.astype(F32), jnp.where(at == 1, low.astype(F32), 0.0))
        send_ref[VAL_DIM:, :] = both.astype(BF16)


def read_sent(ref):
    state = ref[0:VAL_DIM, :].astype(F32)
    tail = ref[VAL_DIM:, :].astype(F32)
    return state, tail[0:1, :] + tail[1:2, :]


def read_state(ref):
    return ref[0:VAL_DIM, :], ref[VAL_DIM : VAL_DIM + 1, :]


def chain(earlier, later):
    return jnp.exp(later[1]) * earlier[0] + later[0], earlier[1] + later[1]


STATE = jax.ShapeDtypeStruct((VAL_DIM + 8, KEY_DIM), F32)
SENT = jax.ShapeDtypeStruct((VAL_DIM + 16, KEY_DIM), BF16)


def linear_local(q, k, v, d):
    return pl.pallas_call(
        linear_kernel,
        out_shape=(
            jax.ShapeDtypeStruct((TOK, VAL_DIM), F32),
            jax.ShapeDtypeStruct((TOK, KEY_DIM), BF16),
            STATE,
            SENT,
        ),
        in_specs=[vmem()] * 4,
        out_specs=(vmem(),) * 4,
        cost_estimate=pl.CostEstimate(
            flops=3_000_000_000, bytes_accessed=800_000, transcendentals=0
        ),
        compiler_params=params(8),
        name="linear_local",
    )(q, k, v, d)


def pair_kernel(me_ref, own_ref, got_ref, all_ref, before_ref, send_ref):
    second = (me_ref[0] & 1) == 1
    own, got = read_state(own_ref), read_sent(got_ref)
    first_s = jnp.where(second, got[0], own[0])
    first_d = jnp.where(second, got[1], own[1])
    later_s = jnp.where(second, own[0], got[0])
    later_d = jnp.where(second, own[1], got[1])
    state, passed = chain((first_s, first_d), (later_s, later_d))
    write_state(state, passed, all_ref, send_ref)
    write_state(
        jnp.where(second, got[0], 0.0), jnp.where(second, got[1], 0.0), before_ref, None
    )


def step_kernel(all_ref, before_ref, got_ref, new_all_ref, new_before_ref, send_ref):
    got = read_sent(got_ref)
    state, passed = chain(got, read_state(all_ref))
    write_state(state, passed, new_all_ref, send_ref)
    state, passed = chain(got, read_state(before_ref))
    write_state(state, passed, new_before_ref, None)


def small_cost():
    return pl.CostEstimate(flops=500_000_000, bytes_accessed=500_000, transcendentals=0)


def pair_state(me, own, got):
    return pl.pallas_call(
        pair_kernel,
        out_shape=(STATE, STATE, SENT),
        in_specs=[smem(), vmem(), vmem()],
        out_specs=(vmem(),) * 3,
        compiler_params=params(8),
        cost_estimate=small_cost(),
        name="pair_state",
    )(me, own, got)


def step_state(whole, before, got):
    return pl.pallas_call(
        step_kernel,
        out_shape=(STATE, STATE, SENT),
        in_specs=[vmem()] * 3,
        out_specs=(vmem(),) * 3,
        compiler_params=params(8),
        cost_estimate=small_cost(),
        name="step_state",
    )(whole, before, got)


ROWS = 2 * TOK
WIDE = 4 * TOK


def attend_kernel(tables, first, off, n_buf, me_ref, qo_ref, qw_ref, *refs):
    bufs = refs[:n_buf]
    if first:
        acc_ref, stat_ref, q_ref, kv_ref, top_ref, part_ref, flag_ref, sems = refs[n_buf:]
    else:
        acc_in, stat_in, acc_ref, stat_ref, q_ref, kv_ref, top_ref, part_ref, flag_ref, sems = refs[
            n_buf:
        ]
    tile = pl.program_id(0) + off
    lead = pl.program_id(0) == 0
    me = me_ref[0]
    z, y, c = me >> 3, (me >> 1) & 3, me & 1
    chip = z * NY + y
    n_group = len(tables)
    pieces = len(tables[0][0])

    def fetches(g):
        if first:
            return [pltpu.make_async_copy(bufs[0], kv_ref.at[0], sems.at[0])]
        per = n_buf // n_group
        rows = WIDE // per
        return [
            pltpu.make_async_copy(
                bufs[g * per + i], kv_ref.at[g, pl.ds(i * rows, rows)], sems.at[g * per + i]
            )
            for i in range(per)
        ]

    @pl.when(lead)
    def _():
        for g, (zero, one) in enumerate(tables):
            for i in range(pieces):
                dz = jnp.where(c == 0, zero[i][0], one[i][0])
                dy = jnp.where(c == 0, zero[i][1], one[i][1])
                source = ((z + dz) & (NZ - 1)) * NY + ((y + dy) & (NY - 1))
                flag_ref[g * pieces + i] = (source < chip).astype(jnp.int32)
            for copy in fetches(g):
                copy.start()

    @pl.when(tile == 0)
    def _():
        q_ref[0:TOK, :] = qo_ref[:, 0:256]
        q_ref[TOK:ROWS, :] = qo_ref[:, 256:512]

    @pl.when(tile == 1)
    def _():
        q_ref[0:TOK, :] = qw_ref[:, 0:256]
        q_ref[TOK:ROWS, :] = qw_ref[:, 256:512]

    lane = lax.broadcasted_iota(jnp.int32, (ROWS, 128), 1)
    if first:
        acc_ref[...] = jnp.zeros_like(acc_ref)
        top_ref[...] = jnp.full(top_ref.shape, NEG, F32)
        part_ref[...] = jnp.zeros_like(part_ref)
    else:
        acc_ref[...] = acc_in[...]
        for mp in range(2):
            top_ref[mp] = jnp.broadcast_to(stat_in[:, mp : mp + 1], (ROWS, 128))
            part_ref[mp] = jnp.where(lane == 0, stat_in[:, 2 + mp : 3 + mp], 0.0)

    def visit(g, lo, n, allowed=None):
        scores = [
            lax.dot_general(
                q_ref[:, mp * 128 : mp * 128 + 128],
                kv_ref[g, pl.ds(lo, n), mp * 128 : mp * 128 + 128],
                NT,
                preferred_element_type=F32,
            )
            for mp in range(2)
        ]
        v = kv_ref[g, pl.ds(lo, n), 256:512]
        for mp in range(2):
            s = scores[mp]
            if allowed is not None:
                s = jnp.where(allowed, s, NEG)
            old = top_ref[mp]
            new = jnp.maximum(old, jnp.max(s, axis=-1, keepdims=True))
            weights, part = [], None
            for j in range(n // 128):
                w = jnp.exp2((s[:, j * 128 : j * 128 + 128] - new) * SCORE)
                part = w if part is None else part + w
                weights.append(w.astype(BF16))
            shrink = jnp.exp2((old - new) * SCORE)
            part_ref[mp] = part_ref[mp] * shrink + part
            top_ref[mp] = new
            added = jnp.dot(
                jnp.concatenate(weights, axis=1), v, preferred_element_type=F32
            )
            for j in range(2):
                cols = slice(mp * 256 + j * 128, mp * 256 + j * 128 + 128)
                acc_ref[:, cols] = acc_ref[:, cols] * shrink + added[:, j * 128 : j * 128 + 128]

    def group(g, lo, n):
        flags = [flag_ref[g * pieces + i] for i in range(pieces)]
        count = functools.reduce(jnp.add, flags)

        @pl.when(count == pieces)
        def _():
            visit(g, lo, n)

        @pl.when((count > 0) & (count < pieces))
        def _():
            def one(i, carry):
                @pl.when(flag_ref[g * pieces + i] != 0)
                def _():
                    visit(g, pl.multiple_of(lo + i * TOK, TOK), TOK)

                return carry

            lax.fori_loop(0, pieces, one, 0)

    def wait(g):
        @pl.when(lead)
        def _():
            for copy in fetches(g):
                copy.wait()

    if first:
        wait(0)
        qb = jnp.where(tile == 0, 1 - c, c)
        row = lax.broadcasted_iota(jnp.int32, (ROWS, TOK), 0) & (TOK - 1)
        col = lax.broadcasted_iota(jnp.int32, (ROWS, TOK), 1)
        visit(0, 0, TOK, allowed=qb * TOK + row >= c * TOK + col)
        group(0, TOK, pieces * TOK)
    else:
        if n_group == 1:
            wait(0)
            group(0, 0, WIDE)
        else:

            def loop(g, carry):
                for which in range(n_group):
                    pl.when(g == which)(functools.partial(wait, which))
                group(g, 0, WIDE)
                return carry

            lax.fori_loop(0, n_group, loop, 0)

    stat_ref[...] = jnp.where(
        lane == 0,
        top_ref[0],
        jnp.where(
            lane == 1,
            top_ref[1],
            jnp.where(
                lane == 2,
                jnp.sum(part_ref[0], axis=-1, keepdims=True),
                jnp.sum(part_ref[1], axis=-1, keepdims=True),
            ),
        ),
    )


def attend(me, qo, qw, bufs, tables, state=None, off=0, tiles=2):
    first = state is None
    n_group = len(tables)
    keys = WIDE * n_group
    acc = lambda o: pl.BlockSpec((ROWS, 512), lambda t: (t + o, 0))
    stat = lambda o: pl.BlockSpec((ROWS, 128), lambda t: (t + o, 0))
    return pl.pallas_call(
        functools.partial(attend_kernel, tables, first, off, len(bufs)),
        grid=(tiles,),
        out_shape=(
            jax.ShapeDtypeStruct((tiles * ROWS, 512), F32),
            jax.ShapeDtypeStruct((tiles * ROWS, 128), F32),
        ),
        in_specs=[
            smem(),
            vmem(),
            vmem(),
            *[any_space()] * len(bufs),
            *([] if first else [acc(off), stat(off)]),
        ],
        out_specs=(acc(0), stat(0)),
        scratch_shapes=[
            pltpu.VMEM((ROWS, 256), BF16),
            pltpu.VMEM((n_group, WIDE, 512), BF16),
            pltpu.VMEM((2, ROWS, 128), F32),
            pltpu.VMEM((2, ROWS, 128), F32),
            pltpu.SMEM((n_group * len(tables[0][0]),), jnp.int32),
            pltpu.SemaphoreType.DMA((len(bufs),)),
        ],
        compiler_params=params(20, dimension_semantics=("arbitrary",)),
        cost_estimate=pl.CostEstimate(
            flops=2 * tiles * ROWS * keys * 2 * (256 + 256),
            bytes_accessed=4_000_000,
            transcendentals=0,
        ),
        name="attend",
    )(me, qo, qw, *bufs, *(() if first else state))


CUTS = 8


def head_norm(x, gain):
    return x * lax.rsqrt(jnp.mean(x * x, axis=-1, keepdims=True) + EPS) * gain


def project_kernel(
    lam_ref, acc_hbm, oacc_hbm, wd_hbm, wl_hbm, stat_ref, ostat_ref, dg_ref, rows_ref, reach_ref,
    before_ref, got_ref, lg_ref, out_hbm, acc_ref, oacc_ref, w_ref, x_ref, o_ref, sems,
):
    width = w_ref.shape[1] // CUTS
    load = [
        pltpu.make_async_copy(acc_hbm, acc_ref, sems.at[0]),
        pltpu.make_async_copy(oacc_hbm, oacc_ref, sems.at[1]),
    ]
    weights = []
    for j in range(CUTS):
        cols = pl.ds(j * width, width)
        weights.append(
            (
                pltpu.make_async_copy(
                    wd_hbm.at[:, cols], w_ref.at[0:512, cols], sems.at[2 + 2 * j]
                ),
                pltpu.make_async_copy(
                    wl_hbm.at[:, cols], w_ref.at[512:768, cols], sems.at[3 + 2 * j]
                ),
            )
        )
    for copy in load:
        copy.start()
    for pair in weights:
        for copy in pair:
            copy.start()
    incoming, _ = chain(read_sent(got_ref), read_state(before_ref))
    linear = rows_ref[...] + lax.dot_general(
        reach_ref[...], incoming.astype(BF16), NT, preferred_element_type=F32
    )
    x_ref[:, 512:768] = head_norm(linear, lg_ref[...]).astype(BF16)
    for copy in load:
        copy.wait()
    for h in range(2):
        maps = []
        part = slice(h * TOK, h * TOK + TOK)
        for mp in range(2):
            top_a, top_b = stat_ref[part, mp : mp + 1], ostat_ref[part, mp : mp + 1]
            top = jnp.maximum(top_a, top_b)
            sa = jnp.exp2((top_a - top) * SCORE)
            sb = jnp.exp2((top_b - top) * SCORE)
            total = stat_ref[part, 2 + mp : 3 + mp] * sa + ostat_ref[part, 2 + mp : 3 + mp] * sb
            cols = slice(mp * 256, mp * 256 + 256)
            maps.append(acc_ref[part, cols] * (sa / total) + oacc_ref[part, cols] * (sb / total))
        attended = maps[0] - lam_ref[h] * maps[1]
        x_ref[:, h * 256 : h * 256 + 256] = head_norm(attended, dg_ref[...]).astype(BF16)
    stores = []
    for j, pair in enumerate(weights):
        for copy in pair:
            copy.wait()
        cols = slice(j * width, j * width + width)
        o_ref[j] = jnp.dot(x_ref[...], w_ref[:, cols], preferred_element_type=F32).astype(BF16)
        store = pltpu.make_async_copy(
            o_ref.at[j], out_hbm.at[:, pl.ds(j * width, width)], sems.at[2 + 2 * CUTS + j]
        )
        store.start()
        stores.append(store)
    for store in stores:
        store.wait()


def project(lam, state, other, dg, rows, reach, before, got, lg, wd, wl):
    model = wd.shape[1]
    return pl.pallas_call(
        project_kernel,
        out_shape=jax.ShapeDtypeStruct((TOK, model), BF16),
        in_specs=[smem(), *[any_space()] * 4, *[vmem()] * 8],
        out_specs=any_space(),
        scratch_shapes=[
            pltpu.VMEM((ROWS, 512), F32),
            pltpu.VMEM((ROWS, 512), F32),
            pltpu.VMEM((768, model), BF16),
            pltpu.VMEM((TOK, 768), BF16),
            pltpu.VMEM((CUTS, TOK, model // CUTS), BF16),
            pltpu.SemaphoreType.DMA((2 + 3 * CUTS,)),
        ],
        cost_estimate=pl.CostEstimate(
            flops=2 * TOK * 768 * model, bytes_accessed=12_000_000, transcendentals=0
        ),
        compiler_params=params(24),
        name="project",
    )(lam, state[0], other[0], wd, wl, state[1], other[1], dg, rows, reach, before, got, lg)


ROW = (0, -1, 1, -2)
NEAR = (0, -1, 1, -2)
FAR = (2, -3, 3, 4)


def body(
    queries, keys, values, lam, diff_gain, lin_query, lin_key, lin_value,
    decay_pre, lin_gain, w_out_diff, w_out_lin,
):
    me = lax.axis_index(SP).astype(jnp.int32).reshape(1)
    tied = lax.optimization_barrier
    every = slice(None)
    span = lambda k: pl.ds(k * TOK, TOK)
    (kv,) = join(
        me,
        (keys, values),
        1,
        TOK,
        (((0, 0, every, pl.ds(0, 256)), (1, 0, every, pl.ds(256, 256))),),
    )
    zp, zm, yp, ym = (1, 0), (-1, 0), (0, 1), (0, -1)

    p1, m1 = moved(kv, zp, yp), moved(kv, zm, ym)
    q_other = swap(queries)
    rows, reach, own_state, sent = linear_local(lin_query, lin_key, lin_value, decay_pre)
    got = swap(sent)
    p1, m1, q_other, own_state, got = tied((p1, m1, q_other, own_state, got))

    p2, m2 = moved(p1, zp, yp), moved(m1, zm, ym)
    whole, before, sent = pair_state(me, own_state, got)
    got = chip_ahead(sent, 1)
    p2, m2, got = tied((p2, m2, got))

    (near,) = join(
        me,
        (kv, p1, m1, p2),
        1,
        WIDE,
        (tuple((i, 0, span(i), every) for i in range(4)),),
    )
    p3, m3 = moved(near, yp, zp), moved(near, ym, zm)
    xm3, xp3 = moved(p2, zp, yp), moved(m2, zm, ym)
    whole, before, sent = step_state(whole, before, got)
    got = chip_ahead(sent, 2)
    state = attend(
        me,
        q_other,
        queries,
        (near,),
        ((tuple((dz, 0) for dz in NEAR[1:]), tuple((0, dy) for dy in ROW[1:])),),
    )
    p3, m3, xm3, xp3, got, state = tied((p3, m3, xm3, xp3, got, state))

    p4, m4 = moved(p3, yp, zp), moved(m3, ym, zm)
    x4 = moved(xm3, zp, yp)
    whole, before, sent = step_state(whole, before, got)
    got = chip_ahead(sent, 4)
    state = attend(
        me,
        q_other,
        queries,
        (p3, m3),
        (
            (tuple((dz, -1) for dz in NEAR), tuple((-1, dy) for dy in ROW)),
            (tuple((dz, 1) for dz in NEAR), tuple((1, dy) for dy in ROW)),
        ),
        state,
    )
    p4, m4, x4, got, state = tied((p4, m4, x4, got, state))

    far_p, far_m = join(
        me,
        (m2, xm3, xp3, x4, p4, m4),
        2,
        WIDE,
        (
            tuple((i, o, span(i), every) for o in range(2) for i in range(4)),
            ((4, 0, every, every), (5, 1, every, every)),
        ),
    )
    p5, m5 = moved(far_p, yp, zp), moved(far_m, ym, zm)
    whole, before, sent = step_state(whole, before, got)
    got = chip_ahead(sent, 8)
    state = attend(
        me,
        q_other,
        queries,
        (p4, far_m),
        (
            (tuple((dz, -2) for dz in NEAR), tuple((-2, dy) for dy in ROW)),
            (tuple((dz, 0) for dz in FAR), tuple((2, dy) for dy in ROW)),
        ),
        state,
    )
    p5, m5, got, state = tied((p5, m5, got, state))

    p6, m6 = moved(p5[: 2 * TOK], yp, zp), moved(m5[2 * TOK :], ym, zm)
    whole, before, sent = step_state(whole, before, got)
    got = chip_ahead(sent, 16)
    state = attend(
        me,
        q_other,
        queries,
        (p5, m5),
        (
            (tuple((dz, -1) for dz in FAR), tuple((-3, dy) for dy in ROW)),
            (tuple((dz, 1) for dz in FAR), tuple((3, dy) for dy in ROW)),
        ),
        state,
    )
    p6, m6, got, state = tied((p6, m6, got, state))

    tail = (
        (p6, m6),
        ((tuple((dz, 2) for dz in FAR), tuple((4, dy) for dy in ROW)),),
    )
    theirs = attend(me, q_other, queries, *tail, state, off=0, tiles=1)
    other = tuple(swap(a) for a in theirs)
    mine = attend(me, q_other, queries, *tail, state, off=1, tiles=1)
    partial = project(
        lam, mine, other, diff_gain.reshape(1, -1), rows, reach, before, got,
        lin_gain.reshape(1, -1), w_out_diff, w_out_lin,
    )
    blocks = partial.reshape(NX, TOK // NX, partial.shape[1])
    arrived = lax.all_to_all(blocks, "tp", split_axis=0, concat_axis=0, tiled=True)
    return arrived.astype(F32).sum(axis=0).astype(BF16)


def solution(mesh):
    finer = Mesh(mesh.devices.reshape(NZ, NY, 2, mesh.shape["tp"]), ("z", "y", "c", "tp"))
    in_specs = (
        P(SP, "tp"),
        P(SP, "tp"),
        P(SP, "tp"),
        P("tp"),
        P(),
        P(SP, "tp"),
        P(SP, "tp"),
        P(SP, "tp"),
        P(SP, "tp"),
        P("tp"),
        P("tp", None),
        P("tp", None),
    )
    out_specs = P((*SP, "tp"), None)
    return jax.shard_map(body, mesh=finer, in_specs=in_specs, out_specs=out_specs, check_vma=False)
```

```python
import functools
import math

import jax
import jax.numpy as jnp
from jax import lax
from jax.experimental import pallas as pl
from jax.experimental.pallas import tpu as pltpu
from jax.sharding import Mesh
from jax.sharding import PartitionSpec as P

HEAD_DIM = 128
KEY_DIM = 128
VAL_DIM = 256
NZ, NY, NX = 8, 4, 4
TOK = 256
HALF = 128
CHIPS = NZ * NY
SP = ("z", "y", "c")
EPS = 1e-6
NEG = -1e30
LOG2E = 1.4426950408889634
SCORE = LOG2E / math.sqrt(HEAD_DIM)
F32 = jnp.float32
BF16 = jnp.bfloat16


NT = (((1,), (1,)), ((), ()))
TN = (((0,), (0,)), ((), ()))


def vmem():
    return pl.BlockSpec(memory_space=pltpu.VMEM)


def smem():
    return pl.BlockSpec(memory_space=pltpu.SMEM)


def hbm():
    return pl.BlockSpec(memory_space=pltpu.HBM)


def params(mib, **kw):
    return pltpu.CompilerParams(vmem_limit_bytes=mib * 2**20, **kw)


def place(z, y, c):
    return (z % NZ) * 8 + (y % NY) * 2 + c


def moved(a, zero=None, one=None):
    pairs = []
    for c, step in ((0, zero), (1, one)):
        if step is not None:
            for z in range(NZ):
                for y in range(NY):
                    pairs.append((place(z, y, c), place(z + step[0], y + step[1], c)))
    return lax.ppermute(a, SP, pairs)


def swap(a):
    return lax.ppermute(a, "c", [(0, 1), (1, 0)])


def chip_ahead(a, d):
    return lax.ppermute(a, ("z", "y"), [(i, i + d) for i in range(CHIPS - d)])


def any_space():
    return pl.BlockSpec(memory_space=pl.ANY)


def join_kernel(plans, n_in, me_ref, *refs):
    ins, outs, sems = refs[:n_in], refs[n_in:-1], refs[-1]

    def run(plan):
        copies = [
            pltpu.make_async_copy(ins[i], outs[o].at[rows, cols], sems.at[k])
            for k, (i, o, rows, cols) in enumerate(plan)
        ]
        for copy in copies:
            copy.start()
        for copy in copies:
            copy.wait()

    if len(plans) == 1:
        run(plans[0])
    else:
        c = me_ref[0] & 1
        for which, plan in enumerate(plans):
            pl.when(c == which)(functools.partial(run, plan))


def join(me, ins, n_out, rows, plans, space=any_space):
    out = jax.ShapeDtypeStruct((rows, 512), BF16)
    return pl.pallas_call(
        functools.partial(join_kernel, plans, len(ins)),
        out_shape=(out,) * n_out,
        in_specs=[smem(), *[space()] * len(ins)],
        out_specs=(vmem(),) * n_out,
        scratch_shapes=[pltpu.SemaphoreType.DMA((max(map(len, plans)),))],
        compiler_params=params(8),
        cost_estimate=small_cost(),
        name="join",
    )(me, *ins)


def linear_kernel(
    q_hbm, k_hbm, v_hbm, d_hbm, rows_ref, reach_ref, state_ref, send_ref,
    q_ref, k_ref, v_ref, d_ref, sems,
):
    n = HALF
    loads = [
        pltpu.make_async_copy(src, dst, sems.at[i])
        for i, (src, dst) in enumerate(
            ((d_hbm, d_ref), (q_hbm, q_ref), (k_hbm, k_ref), (v_hbm, v_ref))
        )
    ]
    for load in loads:
        load.start()
    for load in loads:
        load.wait()
    row = lax.broadcasted_iota(jnp.int32, (n, n), 0)
    col = lax.broadcasted_iota(jnp.int32, (n, n), 1)
    lower = row >= col
    tri = jnp.where(lower, 1.0, 0.0).astype(F32)
    state = None
    passed = jnp.zeros((1, KEY_DIM), F32)
    for part in range(TOK // n):
        sl = pl.ds(part * n, n)
        pre = d_ref[sl, :]
        decay = (jnp.minimum(pre, 0.0) - jnp.log1p(jnp.exp(-jnp.abs(pre)))) / 16.0
        total = jnp.dot(tri, decay, precision=lax.Precision.HIGHEST, preferred_element_type=F32)
        mid = total[n // 2 - 1 : n // 2, :]
        last = total[n - 1 : n, :]
        q = q_ref[sl, :].astype(F32) * KEY_DIM**-0.5
        k = k_ref[sl, :].astype(F32)
        v = v_ref[sl, :]
        inner = lax.dot_general(
            (q * jnp.exp(total - mid)).astype(BF16),
            (k * jnp.exp(mid - total)).astype(BF16),
            NT,
            preferred_element_type=F32,
        )
        inner = jnp.where(lower, inner, 0.0)
        rows = jnp.dot(inner.astype(BF16), v, preferred_element_type=F32)
        added = lax.dot_general(
            v, (k * jnp.exp(last - total)).astype(BF16), TN, preferred_element_type=F32
        )
        if state is None:
            state = added
        else:
            rows = rows + lax.dot_general(
                (q * jnp.exp(total)).astype(BF16),
                state.astype(BF16),
                NT,
                preferred_element_type=F32,
            )
            state = state * jnp.exp(last) + added
        rows_ref[sl, :] = rows
        reach_ref[sl, :] = (q * jnp.exp(passed + total)).astype(BF16)
        passed = passed + last
    write_state(state, passed, state_ref, send_ref)


def write_state(state, passed, state_ref, send_ref):
    if state_ref is not None:
        state_ref[0:VAL_DIM, :] = state
        state_ref[VAL_DIM:, :] = jnp.broadcast_to(passed, (8, KEY_DIM))
    if send_ref is not None:
        high = passed.astype(BF16)
        low = (passed - high.astype(F32)).astype(BF16)
        send_ref[0:VAL_DIM, :] = state.astype(BF16)
        at = lax.broadcasted_iota(jnp.int32, (16, KEY_DIM), 0)
        both = jnp.where(at == 0, high.astype(F32), jnp.where(at == 1, low.astype(F32), 0.0))
        send_ref[VAL_DIM:, :] = both.astype(BF16)


def read_sent(ref):
    state = ref[0:VAL_DIM, :].astype(F32)
    tail = ref[VAL_DIM:, :].astype(F32)
    return state, tail[0:1, :] + tail[1:2, :]


def read_state(ref):
    return ref[0:VAL_DIM, :], ref[VAL_DIM : VAL_DIM + 1, :]


def chain(earlier, later):
    return jnp.exp(later[1]) * earlier[0] + later[0], earlier[1] + later[1]


STATE = jax.ShapeDtypeStruct((VAL_DIM + 8, KEY_DIM), F32)
SENT = jax.ShapeDtypeStruct((VAL_DIM + 16, KEY_DIM), BF16)


def linear_local(q, k, v, d):
    return pl.pallas_call(
        linear_kernel,
        out_shape=(
            jax.ShapeDtypeStruct((TOK, VAL_DIM), F32),
            jax.ShapeDtypeStruct((TOK, KEY_DIM), BF16),
            STATE,
            SENT,
        ),
        in_specs=[hbm()] * 4,
        out_specs=(vmem(),) * 4,
        scratch_shapes=[
            pltpu.VMEM((TOK, KEY_DIM), BF16),
            pltpu.VMEM((TOK, KEY_DIM), BF16),
            pltpu.VMEM((TOK, VAL_DIM), BF16),
            pltpu.VMEM((TOK, KEY_DIM), F32),
            pltpu.SemaphoreType.DMA((4,)),
        ],
        cost_estimate=pl.CostEstimate(
            flops=3_000_000_000, bytes_accessed=800_000, transcendentals=0
        ),
        compiler_params=params(8),
        name="linear_local",
    )(q, k, v, d)


def pair_kernel(me_ref, own_ref, got_ref, all_ref, before_ref, send_ref):
    second = (me_ref[0] & 1) == 1
    own, got = read_state(own_ref), read_sent(got_ref)
    first_s = jnp.where(second, got[0], own[0])
    first_d = jnp.where(second, got[1], own[1])
    later_s = jnp.where(second, own[0], got[0])
    later_d = jnp.where(second, own[1], got[1])
    state, passed = chain((first_s, first_d), (later_s, later_d))
    write_state(state, passed, all_ref, send_ref)
    write_state(
        jnp.where(second, got[0], 0.0), jnp.where(second, got[1], 0.0), before_ref, None
    )


def step_kernel(all_ref, before_ref, got_ref, new_all_ref, new_before_ref, send_ref):
    got = read_sent(got_ref)
    state, passed = chain(got, read_state(all_ref))
    write_state(state, passed, new_all_ref, send_ref)
    state, passed = chain(got, read_state(before_ref))
    write_state(state, passed, new_before_ref, None)


def small_cost():
    return pl.CostEstimate(flops=500_000_000, bytes_accessed=500_000, transcendentals=0)


def pair_state(me, own, got):
    return pl.pallas_call(
        pair_kernel,
        out_shape=(STATE, STATE, SENT),
        in_specs=[smem(), vmem(), vmem()],
        out_specs=(vmem(),) * 3,
        compiler_params=params(8),
        cost_estimate=small_cost(),
        name="pair_state",
    )(me, own, got)


def step_state(whole, before, got):
    return pl.pallas_call(
        step_kernel,
        out_shape=(STATE, STATE, SENT),
        in_specs=[vmem()] * 3,
        out_specs=(vmem(),) * 3,
        compiler_params=params(8),
        cost_estimate=small_cost(),
        name="step_state",
    )(whole, before, got)


ROWS = 2 * TOK
WIDE = 4 * TOK


def attend_kernel(tables, first, off, n_buf, me_ref, qo_ref, qw_ref, *refs):
    bufs = refs[:n_buf]
    if first:
        acc_ref, stat_ref, q_ref, kv_ref, top_ref, part_ref, flag_ref, sems = refs[n_buf:]
    else:
        acc_in, stat_in, acc_ref, stat_ref, q_ref, kv_ref, top_ref, part_ref, flag_ref, sems = refs[
            n_buf:
        ]
    tile = pl.program_id(0) + off
    lead = pl.program_id(0) == 0
    me = me_ref[0]
    z, y, c = me >> 3, (me >> 1) & 3, me & 1
    chip = z * NY + y
    n_group = len(tables)
    pieces = len(tables[0][0])

    def fetches(g):
        if first:
            return [pltpu.make_async_copy(bufs[0], kv_ref.at[0], sems.at[0])]
        per = n_buf // n_group
        rows = WIDE // per
        return [
            pltpu.make_async_copy(
                bufs[g * per + i], kv_ref.at[g, pl.ds(i * rows, rows)], sems.at[g * per + i]
            )
            for i in range(per)
        ]

    @pl.when(lead)
    def _():
        for g, (zero, one) in enumerate(tables):
            for i in range(pieces):
                dz = jnp.where(c == 0, zero[i][0], one[i][0])
                dy = jnp.where(c == 0, zero[i][1], one[i][1])
                source = ((z + dz) & (NZ - 1)) * NY + ((y + dy) & (NY - 1))
                flag_ref[g * pieces + i] = (source < chip).astype(jnp.int32)
            for copy in fetches(g):
                copy.start()

    @pl.when(tile == 0)
    def _():
        q_ref[0:TOK, :] = qo_ref[:, 0:256]
        q_ref[TOK:ROWS, :] = qo_ref[:, 256:512]

    @pl.when(tile == 1)
    def _():
        q_ref[0:TOK, :] = qw_ref[:, 0:256]
        q_ref[TOK:ROWS, :] = qw_ref[:, 256:512]

    lane = lax.broadcasted_iota(jnp.int32, (ROWS, 128), 1)
    if first:
        acc_ref[...] = jnp.zeros_like(acc_ref)
        top_ref[...] = jnp.full(top_ref.shape, NEG, F32)
        part_ref[...] = jnp.zeros_like(part_ref)
    else:
        acc_ref[...] = acc_in[...]
        for mp in range(2):
            top_ref[mp] = jnp.broadcast_to(stat_in[:, mp : mp + 1], (ROWS, 128))
            part_ref[mp] = jnp.where(lane == 0, stat_in[:, 2 + mp : 3 + mp], 0.0)

    def visit(g, lo, n, allowed=None):
        scores = [
            lax.dot_general(
                q_ref[:, mp * 128 : mp * 128 + 128],
                kv_ref[g, pl.ds(lo, n), mp * 128 : mp * 128 + 128],
                NT,
                preferred_element_type=F32,
            )
            for mp in range(2)
        ]
        v = kv_ref[g, pl.ds(lo, n), 256:512]
        for mp in range(2):
            s = scores[mp]
            if allowed is not None:
                s = jnp.where(allowed, s, NEG)
            old = top_ref[mp]
            new = jnp.maximum(old, jnp.max(s, axis=-1, keepdims=True))
            weights, part = [], None
            for j in range(n // 128):
                w = jnp.exp2((s[:, j * 128 : j * 128 + 128] - new) * SCORE)
                part = w if part is None else part + w
                weights.append(w.astype(BF16))
            shrink = jnp.exp2((old - new) * SCORE)
            part_ref[mp] = part_ref[mp] * shrink + part
            top_ref[mp] = new
            added = jnp.dot(
                jnp.concatenate(weights, axis=1), v, preferred_element_type=F32
            )
            for j in range(2):
                cols = slice(mp * 256 + j * 128, mp * 256 + j * 128 + 128)
                acc_ref[:, cols] = acc_ref[:, cols] * shrink + added[:, j * 128 : j * 128 + 128]

    def group(g, lo, n):
        flags = [flag_ref[g * pieces + i] for i in range(pieces)]
        count = functools.reduce(jnp.add, flags)

        @pl.when(count == pieces)
        def _():
            visit(g, lo, n)

        @pl.when((count > 0) & (count < pieces))
        def _():
            def one(i, carry):
                @pl.when(flag_ref[g * pieces + i] != 0)
                def _():
                    visit(g, pl.multiple_of(lo + i * TOK, TOK), TOK)

                return carry

            lax.fori_loop(0, pieces, one, 0)

    def wait(g):
        @pl.when(lead)
        def _():
            for copy in fetches(g):
                copy.wait()

    if first:
        wait(0)
        qb = jnp.where(tile == 0, 1 - c, c)
        row = lax.broadcasted_iota(jnp.int32, (ROWS, TOK), 0) & (TOK - 1)
        col = lax.broadcasted_iota(jnp.int32, (ROWS, TOK), 1)
        visit(0, 0, TOK, allowed=qb * TOK + row >= c * TOK + col)
        group(0, TOK, pieces * TOK)
    else:
        if n_group == 1:
            wait(0)
            group(0, 0, WIDE)
        else:

            def loop(g, carry):
                for which in range(n_group):
                    pl.when(g == which)(functools.partial(wait, which))
                group(g, 0, WIDE)
                return carry

            lax.fori_loop(0, n_group, loop, 0)

    stat_ref[...] = jnp.where(
        lane == 0,
        top_ref[0],
        jnp.where(
            lane == 1,
            top_ref[1],
            jnp.where(
                lane == 2,
                jnp.sum(part_ref[0], axis=-1, keepdims=True),
                jnp.sum(part_ref[1], axis=-1, keepdims=True),
            ),
        ),
    )


def attend(me, qo, qw, bufs, tables, state=None, off=0, tiles=2):
    first = state is None
    n_group = len(tables)
    keys = WIDE * n_group
    acc = lambda o: pl.BlockSpec((ROWS, 512), lambda t: (t + o, 0))
    stat = lambda o: pl.BlockSpec((ROWS, 128), lambda t: (t + o, 0))
    return pl.pallas_call(
        functools.partial(attend_kernel, tables, first, off, len(bufs)),
        grid=(tiles,),
        out_shape=(
            jax.ShapeDtypeStruct((tiles * ROWS, 512), F32),
            jax.ShapeDtypeStruct((tiles * ROWS, 128), F32),
        ),
        in_specs=[
            smem(),
            vmem(),
            vmem(),
            *[any_space()] * len(bufs),
            *([] if first else [acc(off), stat(off)]),
        ],
        out_specs=(acc(0), stat(0)),
        scratch_shapes=[
            pltpu.VMEM((ROWS, 256), BF16),
            pltpu.VMEM((n_group, WIDE, 512), BF16),
            pltpu.VMEM((2, ROWS, 128), F32),
            pltpu.VMEM((2, ROWS, 128), F32),
            pltpu.SMEM((n_group * len(tables[0][0]),), jnp.int32),
            pltpu.SemaphoreType.DMA((len(bufs),)),
        ],
        compiler_params=params(20, dimension_semantics=("arbitrary",)),
        cost_estimate=pl.CostEstimate(
            flops=2 * tiles * ROWS * keys * 2 * (256 + 256),
            bytes_accessed=4_000_000,
            transcendentals=0,
        ),
        name="attend",
    )(me, qo, qw, *bufs, *(() if first else state))


SUB = TOK // NX
SIDE = 2048
CUT = 2048
FINE = 512


def weight_loads(wd_hbm, wl_hbm, w_ref, sems):
    loads = []
    for j in range(2 * SIDE // CUT):
        cols = pl.ds(j * CUT, CUT)
        loads.append(
            (
                pltpu.make_async_copy(wd_hbm.at[:, cols], w_ref.at[0:512, cols], sems.at[2 * j]),
                pltpu.make_async_copy(
                    wl_hbm.at[:, cols], w_ref.at[512:768, cols], sems.at[2 * j + 1]
                ),
            )
        )
    for pair in loads:
        for load in pair:
            load.start()
    return loads


def finely(run):
    def one(j, carry):
        run(pl.multiple_of(j * FINE, FINE))
        return carry

    lax.fori_loop(0, SIDE // FINE, one, 0)


def head_norm(x, gain):
    return x * lax.rsqrt(jnp.mean(x * x, axis=-1, keepdims=True) + EPS) * gain


def merge_kernel(
    at_ref, lam_ref, acc_ref, oacc_ref, wd_ref, wl_ref, stat_ref, ostat_ref, dg_ref, rows_ref,
    reach_ref, before_ref, got_ref, lg_ref, *refs,
):
    sides, own_ref, (x_ref, turned_ref, w_ref, sems) = (refs[0:3], refs[3:6]), refs[6], refs[7:]
    loads = weight_loads(wd_ref, wl_ref, w_ref, sems)
    incoming, _ = chain(read_sent(got_ref), read_state(before_ref))
    linear = rows_ref[...] + lax.dot_general(
        reach_ref[...], incoming.astype(BF16), NT, preferred_element_type=F32
    )
    x_ref[:, 512:768] = head_norm(linear, lg_ref[...]).astype(BF16)
    for h in range(2):
        maps = []
        part = slice(h * TOK, h * TOK + TOK)
        for mp in range(2):
            top_a, top_b = stat_ref[part, mp : mp + 1], ostat_ref[part, mp : mp + 1]
            top = jnp.maximum(top_a, top_b)
            sa = jnp.exp2((top_a - top) * SCORE)
            sb = jnp.exp2((top_b - top) * SCORE)
            total = stat_ref[part, 2 + mp : 3 + mp] * sa + ostat_ref[part, 2 + mp : 3 + mp] * sb
            cols = slice(mp * 256, mp * 256 + 256)
            maps.append(acc_ref[part, cols] * (sa / total) + oacc_ref[part, cols] * (sb / total))
        attended = maps[0] - lam_ref[h] * maps[1]
        x_ref[:, h * 256 : h * 256 + 256] = head_norm(attended, dg_ref[...]).astype(BF16)
    for i, r in enumerate((2, 1, 3, 0)):
        block = pl.multiple_of(((at_ref[0] + r) & (NX - 1)) * SUB, SUB)
        turned_ref[i * SUB : i * SUB + SUB, :] = x_ref[pl.ds(block, SUB), :]
    for outs, lo, pair in zip(sides, (0, SIDE), loads):
        for load in pair:
            load.wait()

        def one(at, outs=outs, lo=lo):
            w = w_ref[:, pl.ds(lo + at, FINE)]
            y = jnp.dot(turned_ref[...], w, preferred_element_type=F32)
            for i, out in enumerate(outs):
                out[:, pl.ds(at, FINE)] = y[i * SUB : i * SUB + SUB].astype(BF16)
            own_ref[:, pl.ds(lo + at, FINE)] = y[3 * SUB :]

        finely(one)


def merge(at, lam, state, other, dg, rows, reach, before, got, lg, wd, wl):
    half = jax.ShapeDtypeStruct((SUB, SIDE), BF16)
    return pl.pallas_call(
        merge_kernel,
        out_shape=(half,) * 6 + (jax.ShapeDtypeStruct((SUB, 2 * SIDE), F32),),
        in_specs=[smem(), smem(), vmem(), vmem(), any_space(), any_space(), *[vmem()] * 8],
        out_specs=(vmem(),) * 7,
        scratch_shapes=[
            pltpu.VMEM((TOK, 768), BF16),
            pltpu.VMEM((TOK, 768), BF16),
            pltpu.VMEM((768, 2 * SIDE), BF16),
            pltpu.SemaphoreType.DMA((4,)),
        ],
        compiler_params=params(49),
        cost_estimate=pl.CostEstimate(
            flops=2 * TOK * 768 * 4096, bytes_accessed=12_000_000, transcendentals=0
        ),
        name="merge",
    )(at, lam, state[0], other[0], wd, wl, state[1], other[1], dg, rows, reach, before, got, lg)


def fold_kernel(a_ref, b_ref, c_ref, d_ref, ab_ref, cd_ref):
    def one(at):
        cols = pl.ds(at, FINE)
        ab_ref[:, cols] = (a_ref[:, cols].astype(F32) + b_ref[:, cols].astype(F32)).astype(BF16)
        cd_ref[:, cols] = (c_ref[:, cols].astype(F32) + d_ref[:, cols].astype(F32)).astype(BF16)

    finely(one)


def fold(a, b, c, d):
    half = jax.ShapeDtypeStruct((SUB, SIDE), BF16)
    return pl.pallas_call(
        fold_kernel,
        out_shape=(half, half),
        in_specs=[vmem()] * 4,
        out_specs=(vmem(),) * 2,
        compiler_params=params(8),
        cost_estimate=small_cost(),
        name="fold",
    )(a, b, c, d)


def total_kernel(own_ref, al_ref, ar_ref, bl_ref, br_ref, out_ref):
    def one(at):
        cols = pl.ds(at, FINE)
        for lo, a, b in ((0, al_ref, bl_ref), (SIDE, ar_ref, br_ref)):
            here = pl.ds(lo + at, FINE)
            out_ref[:, here] = (
                own_ref[:, here] + a[:, cols].astype(F32) + b[:, cols].astype(F32)
            ).astype(BF16)

    finely(one)


def total(own, *parts):
    return pl.pallas_call(
        total_kernel,
        out_shape=jax.ShapeDtypeStruct((SUB, 2 * SIDE), BF16),
        in_specs=[vmem()] * 5,
        out_specs=vmem(),
        compiler_params=params(8),
        cost_estimate=small_cost(),
        name="total",
    )(own, *parts)


ROW = (0, -1, 1, -2)
NEAR = (0, -1, 1, -2)
FAR = (2, -3, 3, 4)


def body(
    queries, keys, values, lam, diff_gain, lin_query, lin_key, lin_value,
    decay_pre, lin_gain, w_out_diff, w_out_lin,
):
    me = lax.axis_index(SP).astype(jnp.int32).reshape(1)
    tied = lax.optimization_barrier
    every = slice(None)
    span = lambda k: pl.ds(k * TOK, TOK)
    (kv,) = join(
        me,
        (keys, values),
        1,
        TOK,
        (((0, 0, every, pl.ds(0, 256)), (1, 0, every, pl.ds(256, 256))),),
        hbm,
    )
    zp, zm, yp, ym, stay = (1, 0), (-1, 0), (0, 1), (0, -1), (0, 0)

    p1, m1 = moved(kv, zp, yp), moved(kv, zm, ym)
    q_other = swap(queries)
    rows, reach, own_state, sent = linear_local(lin_query, lin_key, lin_value, decay_pre)
    got = swap(sent)
    p1, m1, q_other, own_state, got = tied((p1, m1, q_other, own_state, got))

    p2, m2 = moved(p1, zp, yp), moved(m1, zm, ym)
    whole, before, sent = pair_state(me, own_state, got)
    got = chip_ahead(sent, 1)
    p2, m2, got = tied((p2, m2, got))

    (near,) = join(
        me,
        (kv, p1, m1, p2),
        1,
        WIDE,
        (tuple((i, 0, span(i), every) for i in range(4)),),
    )
    p3, m3 = moved(near, yp, zp), moved(near, ym, zm)
    xm3, xp3 = moved(p2, zp, stay), moved(m2, zm, stay)
    whole, before, sent = step_state(whole, before, got)
    got = chip_ahead(sent, 2)
    state = attend(
        me,
        q_other,
        queries,
        (near,),
        ((tuple((dz, 0) for dz in NEAR[1:]), tuple((0, dy) for dy in ROW[1:])),),
    )
    p3, m3, xm3, xp3, got, state = tied((p3, m3, xm3, xp3, got, state))

    p4, m4 = moved(p3, yp, zp), moved(m3, ym, zm)
    x4 = moved(xm3, zp, stay)
    whole, before, sent = step_state(whole, before, got)
    got = chip_ahead(sent, 4)
    state = attend(
        me,
        q_other,
        queries,
        (p3, m3),
        (
            (tuple((dz, -1) for dz in NEAR), tuple((-1, dy) for dy in ROW)),
            (tuple((dz, 1) for dz in NEAR), tuple((1, dy) for dy in ROW)),
        ),
        state,
    )
    p4, m4, x4, got, state = tied((p4, m4, x4, got, state))

    far_p, far_m = join(
        me,
        (m2, xm3, xp3, x4, p4, m4),
        2,
        WIDE,
        (
            tuple((i, o, span(i), every) for o in range(2) for i in range(4)),
            ((4, 0, every, every), (5, 1, every, every)),
        ),
    )
    p5, m5 = moved(far_p, yp, zp), moved(far_m, ym, zm)
    whole, before, sent = step_state(whole, before, got)
    got = chip_ahead(sent, 8)
    state = attend(
        me,
        q_other,
        queries,
        (p4, far_m),
        (
            (tuple((dz, -2) for dz in NEAR), tuple((-2, dy) for dy in ROW)),
            (tuple((dz, 0) for dz in FAR), tuple((2, dy) for dy in ROW)),
        ),
        state,
    )
    p5, m5, got, state = tied((p5, m5, got, state))

    p6, m6 = moved(p5[: 2 * TOK], yp, zp), moved(m5[2 * TOK :], ym, zm)
    whole, before, sent = step_state(whole, before, got)
    got = chip_ahead(sent, 16)
    state = attend(
        me,
        q_other,
        queries,
        (p5, m5),
        (
            (tuple((dz, -1) for dz in FAR), tuple((-3, dy) for dy in ROW)),
            (tuple((dz, 1) for dz in FAR), tuple((3, dy) for dy in ROW)),
        ),
        state,
    )
    p6, m6, got, state = tied((p6, m6, got, state))

    tail = (
        (p6, m6),
        ((tuple((dz, 2) for dz in FAR), tuple((4, dy) for dy in ROW)),),
    )
    acc, stat = attend(me, q_other, queries, *tail, state)
    other = swap(acc[:ROWS]), swap(stat[:ROWS])
    mine = acc[ROWS:], stat[ROWS:]
    at = lax.axis_index("tp").astype(jnp.int32).reshape(1)
    left, ahead_l, back_l, right, ahead_r, back_r, own = merge(
        at, lam, mine, other, diff_gain.reshape(1, -1), rows, reach, before, got,
        lin_gain.reshape(1, -1), w_out_diff, w_out_lin,
    )
    ahead = lambda a: lax.ppermute(a, "tp", [(i, (i + 1) % NX) for i in range(NX)])
    back = lambda a: lax.ppermute(a, "tp", [(i, (i - 1) % NX) for i in range(NX)])
    got_l, got_r = ahead(left), back(right)
    from_r, from_l = ahead(ahead_r), back(back_l)
    got_l, got_r = tied((got_l, got_r, own))[:2]
    ahead_l, back_r = fold(ahead_l, got_l, back_r, got_r)
    return total(own, ahead(ahead_l), from_r, from_l, back(back_r))


def solution(mesh):
    finer = Mesh(mesh.devices.reshape(NZ, NY, 2, mesh.shape["tp"]), ("z", "y", "c", "tp"))
    in_specs = (
        P(SP, "tp"),
        P(SP, "tp"),
        P(SP, "tp"),
        P("tp"),
        P(),
        P(SP, "tp"),
        P(SP, "tp"),
        P(SP, "tp"),
        P(SP, "tp"),
        P("tp"),
        P("tp", None),
        P("tp", None),
    )
    out_specs = P((*SP, "tp"), None)
    return jax.shard_map(body, mesh=finer, in_specs=in_specs, out_specs=out_specs, check_vma=False)
```

```python
import functools
import math

import jax
import jax.numpy as jnp
from jax import lax
from jax.experimental import pallas as pl
from jax.experimental.pallas import tpu as pltpu
from jax.sharding import Mesh
from jax.sharding import PartitionSpec as P

HEAD_DIM = 128
KEY_DIM = 128
VAL_DIM = 256
NZ, NY, NX = 8, 4, 4
TOK = 256
HALF = 128
CHIPS = NZ * NY
SP = ("z", "y", "c")
EPS = 1e-6
NEG = -1e30
LOG2E = 1.4426950408889634
SCORE = LOG2E / math.sqrt(HEAD_DIM)
F32 = jnp.float32
BF16 = jnp.bfloat16


NT = (((1,), (1,)), ((), ()))
TN = (((0,), (0,)), ((), ()))


def vmem():
    return pl.BlockSpec(memory_space=pltpu.VMEM)


def smem():
    return pl.BlockSpec(memory_space=pltpu.SMEM)


def hbm():
    return pl.BlockSpec(memory_space=pltpu.HBM)


def params(mib, **kw):
    return pltpu.CompilerParams(vmem_limit_bytes=mib * 2**20, **kw)


def place(z, y, c):
    return (z % NZ) * 8 + (y % NY) * 2 + c


def moved(a, zero=None, one=None):
    pairs = []
    for c, step in ((0, zero), (1, one)):
        if step is not None:
            for z in range(NZ):
                for y in range(NY):
                    pairs.append((place(z, y, c), place(z + step[0], y + step[1], c)))
    return lax.ppermute(a, SP, pairs)


def swap(a):
    return lax.ppermute(a, "c", [(0, 1), (1, 0)])


def chip_ahead(a, d):
    return lax.ppermute(a, ("z", "y"), [(i, i + d) for i in range(CHIPS - d)])


def any_space():
    return pl.BlockSpec(memory_space=pl.ANY)


def join_kernel(plans, n_in, me_ref, *refs):
    ins, outs, sems = refs[:n_in], refs[n_in:-1], refs[-1]

    def run(plan):
        copies = [
            pltpu.make_async_copy(ins[i], outs[o].at[rows, cols], sems.at[k])
            for k, (i, o, rows, cols) in enumerate(plan)
        ]
        for copy in copies:
            copy.start()
        for copy in copies:
            copy.wait()

    if len(plans) == 1:
        run(plans[0])
    else:
        c = me_ref[0] & 1
        for which, plan in enumerate(plans):
            pl.when(c == which)(functools.partial(run, plan))


def join(me, ins, n_out, rows, plans, space=any_space):
    out = jax.ShapeDtypeStruct((rows, 512), BF16)
    return pl.pallas_call(
        functools.partial(join_kernel, plans, len(ins)),
        out_shape=(out,) * n_out,
        in_specs=[smem(), *[space()] * len(ins)],
        out_specs=(vmem(),) * n_out,
        scratch_shapes=[pltpu.SemaphoreType.DMA((max(map(len, plans)),))],
        compiler_params=params(8),
        cost_estimate=small_cost(),
        name="join",
    )(me, *ins)


def linear_kernel(
    q_hbm, k_hbm, v_hbm, d_hbm, rows_ref, reach_ref, state_ref, send_ref,
    q_ref, k_ref, v_ref, d_ref, sems,
):
    n = HALF
    loads = [
        pltpu.make_async_copy(src, dst, sems.at[i])
        for i, (src, dst) in enumerate(
            ((d_hbm, d_ref), (q_hbm, q_ref), (k_hbm, k_ref), (v_hbm, v_ref))
        )
    ]
    for load in loads:
        load.start()
    for load in loads:
        load.wait()
    row = lax.broadcasted_iota(jnp.int32, (n, n), 0)
    col = lax.broadcasted_iota(jnp.int32, (n, n), 1)
    lower = row >= col
    tri = jnp.where(lower, 1.0, 0.0).astype(F32)
    state = None
    passed = jnp.zeros((1, KEY_DIM), F32)
    for part in range(TOK // n):
        sl = pl.ds(part * n, n)
        pre = d_ref[sl, :]
        decay = (jnp.minimum(pre, 0.0) - jnp.log1p(jnp.exp(-jnp.abs(pre)))) / 16.0
        total = jnp.dot(tri, decay, precision=lax.Precision.HIGHEST, preferred_element_type=F32)
        mid = total[n // 2 - 1 : n // 2, :]
        last = total[n - 1 : n, :]
        q = q_ref[sl, :].astype(F32) * KEY_DIM**-0.5
        k = k_ref[sl, :].astype(F32)
        v = v_ref[sl, :]
        inner = lax.dot_general(
            (q * jnp.exp(total - mid)).astype(BF16),
            (k * jnp.exp(mid - total)).astype(BF16),
            NT,
            preferred_element_type=F32,
        )
        inner = jnp.where(lower, inner, 0.0)
        rows = jnp.dot(inner.astype(BF16), v, preferred_element_type=F32)
        added = lax.dot_general(
            v, (k * jnp.exp(last - total)).astype(BF16), TN, preferred_element_type=F32
        )
        if state is None:
            state = added
        else:
            rows = rows + lax.dot_general(
                (q * jnp.exp(total)).astype(BF16),
                state.astype(BF16),
                NT,
                preferred_element_type=F32,
            )
            state = state * jnp.exp(last) + added
        rows_ref[sl, :] = rows
        reach_ref[sl, :] = (q * jnp.exp(passed + total)).astype(BF16)
        passed = passed + last
    write_state(state, passed, state_ref, send_ref)


def write_state(state, passed, state_ref, send_ref):
    if state_ref is not None:
        state_ref[0:VAL_DIM, :] = state
        state_ref[VAL_DIM:, :] = jnp.broadcast_to(passed, (8, KEY_DIM))
    if send_ref is not None:
        high = passed.astype(BF16)
        low = (passed - high.astype(F32)).astype(BF16)
        send_ref[0:VAL_DIM, :] = state.astype(BF16)
        at = lax.broadcasted_iota(jnp.int32, (16, KEY_DIM), 0)
        both = jnp.where(at == 0, high.astype(F32), jnp.where(at == 1, low.astype(F32), 0.0))
        send_ref[VAL_DIM:, :] = both.astype(BF16)


def read_sent(ref):
    state = ref[0:VAL_DIM, :].astype(F32)
    tail = ref[VAL_DIM:, :].astype(F32)
    return state, tail[0:1, :] + tail[1:2, :]


def read_state(ref):
    return ref[0:VAL_DIM, :], ref[VAL_DIM : VAL_DIM + 1, :]


def chain(earlier, later):
    return jnp.exp(later[1]) * earlier[0] + later[0], earlier[1] + later[1]


STATE = jax.ShapeDtypeStruct((VAL_DIM + 8, KEY_DIM), F32)
SENT = jax.ShapeDtypeStruct((VAL_DIM + 16, KEY_DIM), BF16)


def linear_local(q, k, v, d):
    return pl.pallas_call(
        linear_kernel,
        out_shape=(
            jax.ShapeDtypeStruct((TOK, VAL_DIM), F32),
            jax.ShapeDtypeStruct((TOK, KEY_DIM), BF16),
            STATE,
            SENT,
        ),
        in_specs=[hbm()] * 4,
        out_specs=(vmem(),) * 4,
        scratch_shapes=[
            pltpu.VMEM((TOK, KEY_DIM), BF16),
            pltpu.VMEM((TOK, KEY_DIM), BF16),
            pltpu.VMEM((TOK, VAL_DIM), BF16),
            pltpu.VMEM((TOK, KEY_DIM), F32),
            pltpu.SemaphoreType.DMA((4,)),
        ],
        cost_estimate=pl.CostEstimate(
            flops=3_000_000_000, bytes_accessed=800_000, transcendentals=0
        ),
        compiler_params=params(8),
        name="linear_local",
    )(q, k, v, d)


def pair_kernel(me_ref, own_ref, got_ref, all_ref, before_ref, send_ref):
    second = (me_ref[0] & 1) == 1
    own, got = read_state(own_ref), read_sent(got_ref)
    first_s = jnp.where(second, got[0], own[0])
    first_d = jnp.where(second, got[1], own[1])
    later_s = jnp.where(second, own[0], got[0])
    later_d = jnp.where(second, own[1], got[1])
    state, passed = chain((first_s, first_d), (later_s, later_d))
    write_state(state, passed, all_ref, send_ref)
    write_state(
        jnp.where(second, got[0], 0.0), jnp.where(second, got[1], 0.0), before_ref, None
    )


def step_kernel(all_ref, before_ref, got_ref, new_all_ref, new_before_ref, send_ref):
    got = read_sent(got_ref)
    state, passed = chain(got, read_state(all_ref))
    write_state(state, passed, new_all_ref, send_ref)
    state, passed = chain(got, read_state(before_ref))
    write_state(state, passed, new_before_ref, None)


def small_cost():
    return pl.CostEstimate(flops=500_000_000, bytes_accessed=500_000, transcendentals=0)


def pair_state(me, own, got):
    return pl.pallas_call(
        pair_kernel,
        out_shape=(STATE, STATE, SENT),
        in_specs=[smem(), vmem(), vmem()],
        out_specs=(vmem(),) * 3,
        compiler_params=params(8),
        cost_estimate=small_cost(),
        name="pair_state",
    )(me, own, got)


def step_state(whole, before, got):
    return pl.pallas_call(
        step_kernel,
        out_shape=(STATE, STATE, SENT),
        in_specs=[vmem()] * 3,
        out_specs=(vmem(),) * 3,
        compiler_params=params(8),
        cost_estimate=small_cost(),
        name="step_state",
    )(whole, before, got)


ROWS = 2 * TOK
WIDE = 4 * TOK


def attend_kernel(tables, first, last, off, n_buf, me_ref, qo_ref, qw_ref, *refs):
    bufs = refs[:n_buf]
    if first:
        acc_ref, stat_ref, q_ref, kv_ref, top_ref, part_ref, flag_ref, sems = refs[n_buf:]
    elif last:
        acc_in, stat_in, oa_ref, os_ref, wa_ref, ws_ref = refs[n_buf : n_buf + 6]
        q_ref, kv_ref, top_ref, part_ref, flag_ref, sems, acc_ref = refs[n_buf + 6 :]
    else:
        acc_in, stat_in, acc_ref, stat_ref, q_ref, kv_ref, top_ref, part_ref, flag_ref, sems = refs[
            n_buf:
        ]
    tile = pl.program_id(0) + off
    lead = pl.program_id(0) == 0
    me = me_ref[0]
    z, y, c = me >> 3, (me >> 1) & 3, me & 1
    chip = z * NY + y
    n_group = len(tables)
    pieces = len(tables[0][0])

    def fetches(g):
        if first:
            return [pltpu.make_async_copy(bufs[0], kv_ref.at[0], sems.at[0])]
        per = n_buf // n_group
        rows = WIDE // per
        return [
            pltpu.make_async_copy(
                bufs[g * per + i], kv_ref.at[g, pl.ds(i * rows, rows)], sems.at[g * per + i]
            )
            for i in range(per)
        ]

    @pl.when(lead)
    def _():
        for g, (zero, one) in enumerate(tables):
            for i in range(pieces):
                dz = jnp.where(c == 0, zero[i][0], one[i][0])
                dy = jnp.where(c == 0, zero[i][1], one[i][1])
                source = ((z + dz) & (NZ - 1)) * NY + ((y + dy) & (NY - 1))
                flag_ref[g * pieces + i] = (source < chip).astype(jnp.int32)
            for copy in fetches(g):
                copy.start()

    @pl.when(tile == 0)
    def _():
        q_ref[0:TOK, :] = qo_ref[:, 0:256]
        q_ref[TOK:ROWS, :] = qo_ref[:, 256:512]

    @pl.when(tile == 1)
    def _():
        q_ref[0:TOK, :] = qw_ref[:, 0:256]
        q_ref[TOK:ROWS, :] = qw_ref[:, 256:512]

    lane = lax.broadcasted_iota(jnp.int32, (ROWS, 128), 1)
    if first:
        acc_ref[...] = jnp.zeros_like(acc_ref)
        top_ref[...] = jnp.full(top_ref.shape, NEG, F32)
        part_ref[...] = jnp.zeros_like(part_ref)
    else:
        acc_ref[...] = acc_in[...]
        for mp in range(2):
            top_ref[mp] = jnp.broadcast_to(stat_in[:, mp : mp + 1], (ROWS, 128))
            part_ref[mp] = jnp.where(lane == 0, stat_in[:, 2 + mp : 3 + mp], 0.0)

    def visit(g, lo, n, allowed=None):
        scores = [
            lax.dot_general(
                q_ref[:, mp * 128 : mp * 128 + 128],
                kv_ref[g, pl.ds(lo, n), mp * 128 : mp * 128 + 128],
                NT,
                preferred_element_type=F32,
            )
            for mp in range(2)
        ]
        v = kv_ref[g, pl.ds(lo, n), 256:512]
        for mp in range(2):
            s = scores[mp]
            if allowed is not None:
                s = jnp.where(allowed, s, NEG)
            old = top_ref[mp]
            new = jnp.maximum(old, jnp.max(s, axis=-1, keepdims=True))
            weights, part = [], None
            for j in range(n // 128):
                w = jnp.exp2((s[:, j * 128 : j * 128 + 128] - new) * SCORE)
                part = w if part is None else part + w
                weights.append(w.astype(BF16))
            shrink = jnp.exp2((old - new) * SCORE)
            part_ref[mp] = part_ref[mp] * shrink + part
            top_ref[mp] = new
            added = jnp.dot(
                jnp.concatenate(weights, axis=1), v, preferred_element_type=F32
            )
            for j in range(2):
                cols = slice(mp * 256 + j * 128, mp * 256 + j * 128 + 128)
                acc_ref[:, cols] = acc_ref[:, cols] * shrink + added[:, j * 128 : j * 128 + 128]

    def group(g, lo, n):
        flags = [flag_ref[g * pieces + i] for i in range(pieces)]
        count = functools.reduce(jnp.add, flags)

        @pl.when(count == pieces)
        def _():
            visit(g, lo, n)

        @pl.when((count > 0) & (count < pieces))
        def _():
            def one(i, carry):
                @pl.when(flag_ref[g * pieces + i] != 0)
                def _():
                    visit(g, pl.multiple_of(lo + i * TOK, TOK), TOK)

                return carry

            lax.fori_loop(0, pieces, one, 0)

    def wait(g):
        @pl.when(lead)
        def _():
            for copy in fetches(g):
                copy.wait()

    if first:
        wait(0)
        qb = jnp.where(tile == 0, 1 - c, c)
        row = lax.broadcasted_iota(jnp.int32, (ROWS, TOK), 0) & (TOK - 1)
        col = lax.broadcasted_iota(jnp.int32, (ROWS, TOK), 1)
        visit(0, 0, TOK, allowed=qb * TOK + row >= c * TOK + col)
        group(0, TOK, pieces * TOK)
    else:
        if n_group == 1:
            wait(0)
            group(0, 0, WIDE)
        else:

            def loop(g, carry):
                for which in range(n_group):
                    pl.when(g == which)(functools.partial(wait, which))
                group(g, 0, WIDE)
                return carry

            lax.fori_loop(0, n_group, loop, 0)

    stat = jnp.where(
        lane == 0,
        top_ref[0],
        jnp.where(
            lane == 1,
            top_ref[1],
            jnp.where(
                lane == 2,
                jnp.sum(part_ref[0], axis=-1, keepdims=True),
                jnp.sum(part_ref[1], axis=-1, keepdims=True),
            ),
        ),
    )
    if last:

        @pl.when(tile == 0)
        def _():
            oa_ref[...] = acc_ref[...]
            os_ref[...] = stat

        @pl.when(tile == 1)
        def _():
            wa_ref[...] = acc_ref[...]
            ws_ref[...] = stat
    else:
        stat_ref[...] = stat


def attend(me, qo, qw, bufs, tables, state=None, off=0, tiles=2, last=False):
    first = state is None
    n_group = len(tables)
    keys = WIDE * n_group
    acc = lambda o: pl.BlockSpec((ROWS, 512), lambda t: (t + o, 0))
    stat = lambda o: pl.BlockSpec((ROWS, 128), lambda t: (t + o, 0))
    return pl.pallas_call(
        functools.partial(attend_kernel, tables, first, last, off, len(bufs)),
        grid=(tiles,),
        out_shape=(
            jax.ShapeDtypeStruct((ROWS if last else tiles * ROWS, 512), F32),
            jax.ShapeDtypeStruct((ROWS if last else tiles * ROWS, 128), F32),
        )
        * (2 if last else 1),
        in_specs=[
            smem(),
            vmem(),
            vmem(),
            *[any_space()] * len(bufs),
            *([] if first else [acc(off), stat(off)]),
        ],
        out_specs=(
            (pl.BlockSpec((ROWS, 512), lambda t: (0, 0)), pl.BlockSpec((ROWS, 128), lambda t: (0, 0)))
            * 2
            if last
            else (acc(0), stat(0))
        ),
        scratch_shapes=[
            pltpu.VMEM((ROWS, 256), BF16),
            pltpu.VMEM((n_group, WIDE, 512), BF16),
            pltpu.VMEM((2, ROWS, 128), F32),
            pltpu.VMEM((2, ROWS, 128), F32),
            pltpu.SMEM((n_group * len(tables[0][0]),), jnp.int32),
            pltpu.SemaphoreType.DMA((len(bufs),)),
            *([pltpu.VMEM((ROWS, 512), F32)] if last else []),
        ],
        compiler_params=params(20, dimension_semantics=("arbitrary",)),
        cost_estimate=pl.CostEstimate(
            flops=2 * tiles * ROWS * keys * 2 * (256 + 256),
            bytes_accessed=4_000_000,
            transcendentals=0,
        ),
        name="attend",
    )(me, qo, qw, *bufs, *(() if first else state))


SUB = TOK // NX
SIDE = 2048
CUT = 2048
FINE = 512


def weight_loads(wd_hbm, wl_hbm, w_ref, sems):
    loads = []
    for j in range(2 * SIDE // CUT):
        cols = pl.ds(j * CUT, CUT)
        loads.append(
            (
                pltpu.make_async_copy(wd_hbm.at[:, cols], w_ref.at[0:512, cols], sems.at[2 * j]),
                pltpu.make_async_copy(
                    wl_hbm.at[:, cols], w_ref.at[512:768, cols], sems.at[2 * j + 1]
                ),
            )
        )
    for pair in loads:
        for load in pair:
            load.start()
    return loads


def finely(run):
    def one(j, carry):
        run(pl.multiple_of(j * FINE, FINE))
        return carry

    lax.fori_loop(0, SIDE // FINE, one, 0)


def head_norm(x, gain):
    return x * lax.rsqrt(jnp.mean(x * x, axis=-1, keepdims=True) + EPS) * gain


def merge_kernel(
    at_ref, lam_ref, acc_ref, oacc_ref, wd_ref, wl_ref, stat_ref, ostat_ref, dg_ref, rows_ref,
    reach_ref, before_ref, got_ref, lg_ref, *refs,
):
    sides, own_ref, (x_ref, turned_ref, w_ref, sems) = (refs[0:3], refs[3:6]), refs[6], refs[7:]
    loads = weight_loads(wd_ref, wl_ref, w_ref, sems)
    incoming, _ = chain(read_sent(got_ref), read_state(before_ref))
    linear = rows_ref[...] + lax.dot_general(
        reach_ref[...], incoming.astype(BF16), NT, preferred_element_type=F32
    )
    x_ref[:, 512:768] = head_norm(linear, lg_ref[...]).astype(BF16)
    for h in range(2):
        maps = []
        part = slice(h * TOK, h * TOK + TOK)
        for mp in range(2):
            top_a, top_b = stat_ref[part, mp : mp + 1], ostat_ref[part, mp : mp + 1]
            top = jnp.maximum(top_a, top_b)
            sa = jnp.exp2((top_a - top) * SCORE)
            sb = jnp.exp2((top_b - top) * SCORE)
            total = stat_ref[part, 2 + mp : 3 + mp] * sa + ostat_ref[part, 2 + mp : 3 + mp] * sb
            cols = slice(mp * 256, mp * 256 + 256)
            maps.append(acc_ref[part, cols] * (sa / total) + oacc_ref[part, cols] * (sb / total))
        attended = maps[0] - lam_ref[h] * maps[1]
        x_ref[:, h * 256 : h * 256 + 256] = head_norm(attended, dg_ref[...]).astype(BF16)
    for i, r in enumerate((2, 1, 3, 0)):
        block = pl.multiple_of(((at_ref[0] + r) & (NX - 1)) * SUB, SUB)
        turned_ref[i * SUB : i * SUB + SUB, :] = x_ref[pl.ds(block, SUB), :]
    for outs, lo, pair in zip(sides, (0, SIDE), loads):
        for load in pair:
            load.wait()

        def one(at, outs=outs, lo=lo):
            w = w_ref[:, pl.ds(lo + at, FINE)]
            y = jnp.dot(turned_ref[...], w, preferred_element_type=F32)
            for i, out in enumerate(outs):
                out[:, pl.ds(at, FINE)] = y[i * SUB : i * SUB + SUB].astype(BF16)
            own_ref[:, pl.ds(lo + at, FINE)] = y[3 * SUB :]

        finely(one)


def merge(at, lam, state, other, dg, rows, reach, before, got, lg, wd, wl):
    half = jax.ShapeDtypeStruct((SUB, SIDE), BF16)
    return pl.pallas_call(
        merge_kernel,
        out_shape=(half,) * 6 + (jax.ShapeDtypeStruct((SUB, 2 * SIDE), F32),),
        in_specs=[smem(), smem(), vmem(), vmem(), any_space(), any_space(), *[vmem()] * 8],
        out_specs=(vmem(),) * 7,
        scratch_shapes=[
            pltpu.VMEM((TOK, 768), BF16),
            pltpu.VMEM((TOK, 768), BF16),
            pltpu.VMEM((768, 2 * SIDE), BF16),
            pltpu.SemaphoreType.DMA((4,)),
        ],
        compiler_params=params(49),
        cost_estimate=pl.CostEstimate(
            flops=2 * TOK * 768 * 4096, bytes_accessed=12_000_000, transcendentals=0
        ),
        name="merge",
    )(at, lam, state[0], other[0], wd, wl, state[1], other[1], dg, rows, reach, before, got, lg)


def fold_kernel(a_ref, b_ref, c_ref, d_ref, ab_ref, cd_ref):
    def one(at):
        cols = pl.ds(at, FINE)
        ab_ref[:, cols] = (a_ref[:, cols].astype(F32) + b_ref[:, cols].astype(F32)).astype(BF16)
        cd_ref[:, cols] = (c_ref[:, cols].astype(F32) + d_ref[:, cols].astype(F32)).astype(BF16)

    finely(one)


def fold(a, b, c, d):
    half = jax.ShapeDtypeStruct((SUB, SIDE), BF16)
    return pl.pallas_call(
        fold_kernel,
        out_shape=(half, half),
        in_specs=[vmem()] * 4,
        out_specs=(vmem(),) * 2,
        compiler_params=params(8),
        cost_estimate=small_cost(),
        name="fold",
    )(a, b, c, d)


def total_kernel(own_ref, al_ref, ar_ref, bl_ref, br_ref, out_ref):
    def one(at):
        cols = pl.ds(at, FINE)
        for lo, a, b in ((0, al_ref, bl_ref), (SIDE, ar_ref, br_ref)):
            here = pl.ds(lo + at, FINE)
            out_ref[:, here] = (
                own_ref[:, here] + a[:, cols].astype(F32) + b[:, cols].astype(F32)
            ).astype(BF16)

    finely(one)


def total(own, *parts):
    return pl.pallas_call(
        total_kernel,
        out_shape=jax.ShapeDtypeStruct((SUB, 2 * SIDE), BF16),
        in_specs=[vmem()] * 5,
        out_specs=vmem(),
        compiler_params=params(8),
        cost_estimate=small_cost(),
        name="total",
    )(own, *parts)


ROW = (0, -1, 1, -2)
NEAR = (0, -1, 1, -2)
FAR = (2, -3, 3, 4)


def body(
    queries, keys, values, lam, diff_gain, lin_query, lin_key, lin_value,
    decay_pre, lin_gain, w_out_diff, w_out_lin,
):
    me = lax.axis_index(SP).astype(jnp.int32).reshape(1)
    tied = lax.optimization_barrier
    every = slice(None)
    span = lambda k: pl.ds(k * TOK, TOK)
    (kv,) = join(
        me,
        (keys, values),
        1,
        TOK,
        (((0, 0, every, pl.ds(0, 256)), (1, 0, every, pl.ds(256, 256))),),
        hbm,
    )
    zp, zm, yp, ym, stay = (1, 0), (-1, 0), (0, 1), (0, -1), (0, 0)

    p1, m1 = moved(kv, zp, yp), moved(kv, zm, ym)
    q_other = swap(queries)
    rows, reach, own_state, sent = linear_local(lin_query, lin_key, lin_value, decay_pre)
    got = swap(sent)
    p1, m1, q_other, own_state, got = tied((p1, m1, q_other, own_state, got))

    p2, m2 = moved(p1, zp, yp), moved(m1, zm, ym)
    whole, before, sent = pair_state(me, own_state, got)
    got = chip_ahead(sent, 1)
    p2, m2, got = tied((p2, m2, got))

    (near,) = join(
        me,
        (kv, p1, m1, p2),
        1,
        WIDE,
        (tuple((i, 0, span(i), every) for i in range(4)),),
    )
    p3, m3 = moved(near, yp, zp), moved(near, ym, zm)
    xm3, xp3 = moved(p2, zp, stay), moved(m2, zm, stay)
    whole, before, sent = step_state(whole, before, got)
    got = chip_ahead(sent, 2)
    state = attend(
        me,
        q_other,
        queries,
        (near,),
        ((tuple((dz, 0) for dz in NEAR[1:]), tuple((0, dy) for dy in ROW[1:])),),
    )
    p3, m3, xm3, xp3, got, state = tied((p3, m3, xm3, xp3, got, state))

    p4, m4 = moved(p3, yp, zp), moved(m3, ym, zm)
    x4 = moved(xm3, zp, stay)
    whole, before, sent = step_state(whole, before, got)
    got = chip_ahead(sent, 4)
    state = attend(
        me,
        q_other,
        queries,
        (p3, m3),
        (
            (tuple((dz, -1) for dz in NEAR), tuple((-1, dy) for dy in ROW)),
            (tuple((dz, 1) for dz in NEAR), tuple((1, dy) for dy in ROW)),
        ),
        state,
    )
    p4, m4, x4, got, state = tied((p4, m4, x4, got, state))

    far_p, far_m = join(
        me,
        (m2, xm3, xp3, x4, p4, m4),
        2,
        WIDE,
        (
            tuple((i, o, span(i), every) for o in range(2) for i in range(4)),
            ((4, 0, every, every), (5, 1, every, every)),
        ),
    )
    p5, m5 = moved(far_p, yp, zp), moved(far_m, ym, zm)
    whole, before, sent = step_state(whole, before, got)
    got = chip_ahead(sent, 8)
    state = attend(
        me,
        q_other,
        queries,
        (p4, far_m),
        (
            (tuple((dz, -2) for dz in NEAR), tuple((-2, dy) for dy in ROW)),
            (tuple((dz, 0) for dz in FAR), tuple((2, dy) for dy in ROW)),
        ),
        state,
    )
    p5, m5, got, state = tied((p5, m5, got, state))

    p6, m6 = moved(p5[: 2 * TOK], yp, zp), moved(m5[2 * TOK :], ym, zm)
    whole, before, sent = step_state(whole, before, got)
    got = chip_ahead(sent, 16)
    state = attend(
        me,
        q_other,
        queries,
        (p5, m5),
        (
            (tuple((dz, -1) for dz in FAR), tuple((-3, dy) for dy in ROW)),
            (tuple((dz, 1) for dz in FAR), tuple((3, dy) for dy in ROW)),
        ),
        state,
    )
    p6, m6, got, state = tied((p6, m6, got, state))

    tail = (
        (p6, m6),
        ((tuple((dz, 2) for dz in FAR), tuple((4, dy) for dy in ROW)),),
    )
    out = attend(me, q_other, queries, *tail, state, last=True)
    other = tuple(swap(a) for a in out[:2])
    mine = out[2:]
    at = lax.axis_index("tp").astype(jnp.int32).reshape(1)
    left, ahead_l, back_l, right, ahead_r, back_r, own = merge(
        at, lam, mine, other, diff_gain.reshape(1, -1), rows, reach, before, got,
        lin_gain.reshape(1, -1), w_out_diff, w_out_lin,
    )
    ahead = lambda a: lax.ppermute(a, "tp", [(i, (i + 1) % NX) for i in range(NX)])
    back = lambda a: lax.ppermute(a, "tp", [(i, (i - 1) % NX) for i in range(NX)])
    got_l, got_r = ahead(left), back(right)
    from_r, from_l = ahead(ahead_r), back(back_l)
    got_l, got_r = tied((got_l, got_r, own))[:2]
    ahead_l, back_r = fold(ahead_l, got_l, back_r, got_r)
    return total(own, ahead(ahead_l), from_r, from_l, back(back_r))


def solution(mesh):
    finer = Mesh(mesh.devices.reshape(NZ, NY, 2, mesh.shape["tp"]), ("z", "y", "c", "tp"))
    in_specs = (
        P(SP, "tp"),
        P(SP, "tp"),
        P(SP, "tp"),
        P("tp"),
        P(),
        P(SP, "tp"),
        P(SP, "tp"),
        P(SP, "tp"),
        P(SP, "tp"),
        P("tp"),
        P("tp", None),
        P("tp", None),
    )
    out_specs = P((*SP, "tp"), None)
    return jax.shard_map(body, mesh=finer, in_specs=in_specs, out_specs=out_specs, check_vma=False)
```
